256 devices in a mesh: grp: 2 (over y), sp: 32 (over z, core), tp: 4 (over x).
Axes of the slice: x: 4, y: 2, z: 16, core: 2. Of those that a mesh axis runs over, the one named last changes fastest.
The devices are a block of a 4x16x16 slice.
Arguments:
- resid: bfloat16 [12288, 2048], P(('grp', 'sp', 'tp')), parts along dimension 0, may hold values from -6 to 6
- queries: bfloat16 [12288, 1024], P(('grp', 'sp'), 'tp'), parts along dimension 0, may hold values from -64 to 64
- keys: bfloat16 [12288, 256], P(('grp', 'sp'), 'tp'), parts along dimension 0, may hold values from -64 to 64
- values: bfloat16 [12288, 256], P(('grp', 'sp'), 'tp'), parts along dimension 0, may hold values from -6 to 6
- doc_ids: int32 [12288], P(('grp', 'sp')), parts along dimension 0, may hold values from 0 to 15, never falling along the last dimension, each value on 1 to 768 neighbouring positions
- sink_logits: float32 [16], P('tp'), may hold values from 2 to 6
- out_proj: bfloat16 [1024, 2048], P('tp'), may hold values from -1.5 to 1.5
- norm1_gain: float32 [2048], replicated, may hold values from 0.1 to 1.9
- norm1_bias: float32 [2048], replicated, may hold values from -1.8 to 1.8
- route_ids: int32 [12288, 2], P(('grp', 'sp', 'tp')), parts along dimension 0, may hold values from 0 to 31, all different within a row; in each aligned block of 48 rows (0 to 47, 48 to 95, ...) at most 3 rows name the same one
- route_weights: float32 [12288, 2], P(('grp', 'sp', 'tp')), parts along dimension 0, may hold values from 0.25 to 1
- expert_gate: bfloat16 [32, 2048, 3072], P('sp', None, 'tp'), may hold values from -0.125 to 0.125
- expert_up: bfloat16 [32, 2048, 3072], P('sp', None, 'tp'), may hold values from -0.125 to 0.125
- expert_down: bfloat16 [32, 3072, 2048], P('sp', 'tp'), may hold values from -0.109375 to 0.109375
- norm2_gain: float32 [2048], replicated, may hold values from 0.1 to 1.9
- norm2_bias: float32 [2048], replicated, may hold values from -1.8 to 1.8
Outputs:
- mixed: bfloat16 [12288, 2048], P(('grp', 'sp', 'tp')), parts along dimension 0
The draws below stay inside these ranges and needn't reach their ends.
There are 2 independent parts, one for each index of `grp`. The reference program is written for one: setup_inputs(seed, part) draws one part's arguments, and reference() takes and returns one part's arrays. A program takes and returns all parts, laid end to end along the dimension named above; an argument that names none is the same for every part. Nothing has to cross between parts.
Inputs may be any that keep to these rules, and one draw needn't show every extreme that they name: `route_ids`: among the rows of one device (aligned blocks of 48 tokens) no expert is named more than 3 times, a bound that some block reaches; a token's 2 experts differ.
All inputs are finite; a program needn't handle non-finite values.
Results may differ from the reference program's by a relative error of at most 0.012.
Values may be sent and summed in bfloat16 or wider, within the bound.
A program may use at most 64 MiB of HBM per device.

```python
import math
import jax
import jax.numpy as jnp
import numpy as np
from jax import lax

D = 2048
HEADS = 16
KV_HEADS = 4
HEAD_DIM = 64
ATT_WIDTH = 1024
FF = 3072
TOPK = 2
WINDOW = 128
TOK_DEV = 192
TOK_SUB = 48
TOKENS = 6144
EXPERTS = 32
CAP = 3
DOCS = 16
DOC_MOST = 768
N_TP = 4


def draw_keys(key, part):
    noise = jnp.clip(jax.random.normal(jax.random.fold_in(key, 1), (TOKENS, KV_HEADS, HEAD_DIM), jnp.float32), -6.0, 6.0)
    return noise.reshape(TOKENS, KV_HEADS * HEAD_DIM).astype(jnp.bfloat16)


def draw_queries(key, part):
    noise = jnp.clip(jax.random.normal(jax.random.fold_in(key, 2), (TOKENS, HEADS, HEAD_DIM), jnp.float32), -6.0, 6.0)
    return noise.reshape(TOKENS, HEADS * HEAD_DIM).astype(jnp.bfloat16)


def block_levels(key, dims, cuts, smallest, high):
    gain, own = 1.0, jax.random.fold_in(key, 6)
    for dim, parts in cuts:
        draws = jnp.exp(jax.random.uniform(jax.random.fold_in(own, dim), (parts,), jnp.float32, smallest / len(cuts), high / len(cuts)))
        gain = gain * jnp.repeat(draws, dims[dim] // parts).reshape([-1 if axis == dim else 1 for axis in range(len(dims))])
    return gain


def profile(number_of, total, most, slope):
    weights = [(1 << 20) // math.isqrt(standing ** slope) + 1 for standing in range(2, number_of + 1)]
    surplus, holding = total - most - (number_of - 1), [1] * (number_of - 1)
    while surplus > 0:
        free = [i for i in range(number_of - 1) if holding[i] < most]
        whole, budget = sum([weights[i] for i in free]), surplus
        for i in free:
            extra = min(most - holding[i], max(1, budget * weights[i] // whole), surplus)
            holding[i] = holding[i] + extra
            surplus = surplus - extra
    return np.array([most] + holding)


def uneven(rng, amount, total, most, lean):
    if amount == 2:
        one = jax.random.randint(rng, (), max(1, total - most), min(most, total - 1) + 1)
        return jnp.stack([one, total - one])
    lengths = jnp.asarray(profile(amount, total, most, lean), jnp.int32)
    pairs = (amount - 1) // 2
    source_of, sink = lengths[1:1 + 2 * pairs:2], lengths[2:2 + 2 * pairs:2]
    room = jnp.minimum(source_of - 1, most - sink)
    moved = jax.random.randint(jax.random.fold_in(rng, 1), (pairs,), 0, 1 << 20) % (room + 1)
    lengths = lengths.at[1:1 + 2 * pairs:2].set(source_of - moved).at[2:2 + 2 * pairs:2].set(sink + moved)
    return lengths[jax.random.permutation(jax.random.fold_in(rng, 2), amount)]


def assign_block(rng, own, number, rows, count, top, most, skew):
    sequence = jax.random.permutation(rng, count)
    packed, usual = load_shares(count, rows * top, most, skew, True), load_shares(count, rows * top, most, skew, False)
    places = jnp.arange(count)

    def named(sizes, rotation):
        used = int((sizes > 0).sum())
        fixed = max(1, used // 4)
        moved = fixed + (places - fixed + rotation * (used - fixed)) % max(1, count - fixed)
        return jnp.zeros((count,), jnp.int32).at[sequence[jnp.where(places < fixed, places, moved)]].set(jnp.asarray(sizes, jnp.int32))

    sizes = jnp.where(number % 4 == 0, named(packed, number // 4), named(usual, number - number // 4 - 1))
    mixed = jax.random.permutation(jax.random.fold_in(own, 3), count)
    donor, sink = mixed[0:count // 2 * 2:2], mixed[1:count // 2 * 2:2]
    room = jnp.minimum(sizes[donor] - 1, most - sizes[sink]) // 2
    room = jnp.where((donor == sequence[0]) | (sink == sequence[0]) | (sizes[sink] == 0), 0, jnp.maximum(room, 0))
    moved = jax.random.randint(jax.random.fold_in(own, 4), (count // 2,), 0, 1 << 20) % (room + 1)
    sizes = sizes.at[donor].add(-moved).at[sink].add(moved)
    labels = jnp.searchsorted(jnp.cumsum(sizes), jnp.arange(rows * top), side="right").astype(jnp.int32)
    grid = labels.reshape(top, rows).T
    grid = grid[jax.random.permutation(jax.random.fold_in(own, 1), rows)]
    rotation = jax.random.randint(jax.random.fold_in(own, 2), (rows, 1), 0, top)
    return jnp.take_along_axis(grid, (jnp.arange(top)[None, :] + rotation) % top, axis=1)


def load_shares(amount, total, limit, skew, full):
    weights = [(1 << 20) // math.isqrt(grade ** skew) + 1 for grade in range(1, amount + 1)]
    largest = limit if full else min(limit, max(-(-total // amount), total * weights[0] // sum(weights)))
    least = 1 if total - largest >= amount - 1 else 0
    given, rest = [largest] + [least] * (amount - 1), total - largest - least * (amount - 1)
    while rest > 0:
        free = [i for i in range(1, amount) if given[i] < largest] or [i for i in range(1, amount) if given[i] < limit]
        mass, budget = sum([weights[i] for i in free]), rest
        for i in free:
            extra = min(limit - given[i], max(1, budget * weights[i] // mass), rest)
            given[i] = given[i] + extra
            rest = rest - extra
    return np.array(given)


def normal_values(own_key, extent, spread, most, shards=(), held_as=jnp.bfloat16):
    values = jax.random.normal(own_key, extent, jnp.float32) * spread
    if len(shards) > 0:
        values = block_levels(own_key, extent, shards, -0.22, 0.18) * values
    return jnp.clip(values, min=-most, max=most).astype(held_as)


def setup_inputs(seed: int = 0, part: int = 0) -> dict:
    seeds = jax.random.split(jax.random.key(seed), 17)
    part_keys = jax.random.split(jax.random.fold_in(seeds[16], part), 17)
    resid = normal_values(part_keys[0], (TOKENS, D), 1.0, 6.0, ((0, 128),))
    queries = draw_queries(jax.random.fold_in(jax.random.fold_in(seeds[16], part), 71), part)
    keys = draw_keys(jax.random.fold_in(jax.random.fold_in(seeds[16], part), 71), part)
    values = normal_values(part_keys[3], (TOKENS, KV_HEADS * HEAD_DIM), 1.0, 6.0, ((0, 32), (1, 4)))
    doc_ids = jnp.searchsorted(jnp.cumsum(uneven(part_keys[4], DOCS, TOKENS, DOC_MOST, 2)), jnp.arange(TOKENS), side="right").astype(jnp.int32)
    sink_logits = jnp.clip(2.0 + 4.0 * jax.random.uniform(seeds[5], (HEADS,), jnp.float32) ** block_levels(seeds[5], (HEADS,), ((0, 4),), -0.2, 0.2), 2.0, 6.0)
    out_proj = normal_values(seeds[6], (ATT_WIDTH, D), (HEAD_DIM // 4) ** -0.5, 1.5, ((0, 4),))
    norm1_gain = jnp.clip(1.0 + 0.18 * jax.random.normal(seeds[7], (D,), jnp.float32), 0.1, 1.9)
    norm1_bias = normal_values(seeds[8], (D,), 0.3, 1.8, (), jnp.float32)
    route_ids_keys = jax.random.split(jax.random.fold_in(part_keys[9], 1), TOKENS // TOK_SUB)
    route_ids_turns = jax.random.permutation(jax.random.fold_in(part_keys[9], 3), TOKENS // TOK_SUB)
    route_ids = jax.vmap(lambda own, number: assign_block(jax.random.fold_in(part_keys[9], 2), own, number, TOK_SUB, EXPERTS, TOPK, CAP, 1))(route_ids_keys, route_ids_turns).reshape((TOKENS, TOPK))
    route_weights = jnp.clip(0.25 + 0.75 * jax.random.uniform(part_keys[10], (TOKENS, TOPK), jnp.float32) ** block_levels(part_keys[10], (TOKENS, TOPK), ((0, 128),), -0.2, 0.2), 0.25, 1.0)
    expert_gate = normal_values(seeds[11], (EXPERTS, D, FF), D ** -0.5, 0.125, ((0, 32), (2, 4)))
    expert_up = normal_values(seeds[12], (EXPERTS, D, FF), D ** -0.5, 0.125, ((0, 32), (2, 4)))
    expert_down = normal_values(seeds[13], (EXPERTS, FF, D), FF ** -0.5, 0.109375, ((0, 32), (1, 4)))
    norm2_gain = jnp.clip(1.0 + 0.18 * jax.random.normal(seeds[14], (D,), jnp.float32), 0.1, 1.9)
    norm2_bias = normal_values(seeds[15], (D,), 0.3, 1.8, (), jnp.float32)
    return {"resid": resid, "queries": queries, "keys": keys, "values": values, "doc_ids": doc_ids, "sink_logits": sink_logits, "out_proj": out_proj, "norm1_gain": norm1_gain, "norm1_bias": norm1_bias, "route_ids": route_ids, "route_weights": route_weights, "expert_gate": expert_gate, "expert_up": expert_up, "expert_down": expert_down, "norm2_gain": norm2_gain, "norm2_bias": norm2_bias}


norm_epsilon = 1e-05
residual_scale = 1.4142135623730951
masked_score = -1e+30

def layer_norm(values, gain_vec, bias_vec):
    mean_val = lax.optimization_barrier(jnp.mean(values, -1, keepdims=True))
    centred = values - mean_val
    variance = lax.optimization_barrier(jnp.mean(centred * centred, -1, keepdims=True))
    return centred * lax.rsqrt(variance + norm_epsilon) * gain_vec + bias_vec

def attention(queries, keys, values, doc_ids, sink_logits):
    groups = HEADS // KV_HEADS
    block = TOK_DEV
    nblocks = TOKENS // block
    reach = block + 2 * WINDOW
    pad_keys = jnp.pad(keys.reshape(TOKENS, KV_HEADS, HEAD_DIM), ((WINDOW, WINDOW), (0, 0), (0, 0)))
    pad_values = jnp.pad(values.reshape(TOKENS, KV_HEADS, HEAD_DIM), ((WINDOW, WINDOW), (0, 0), (0, 0)))
    pad_docs = jnp.pad(doc_ids.astype(jnp.int32), (WINDOW, WINDOW))
    sink_table = sink_logits.astype(jnp.float32).reshape(KV_HEADS, groups, 1, 1)

    def one_block(index):
        start = index * block
        query_blk = lax.dynamic_slice_in_dim(queries, start, block, 0).reshape(block, KV_HEADS, groups, HEAD_DIM)
        key_blk = lax.dynamic_slice_in_dim(pad_keys, start, reach, 0)
        value_blk = lax.dynamic_slice_in_dim(pad_values, start, reach, 0)
        query_docs = lax.dynamic_slice_in_dim(doc_ids.astype(jnp.int32), start, block, 0)
        key_docs = lax.dynamic_slice_in_dim(pad_docs, start, reach, 0)
        query_pos = start + jnp.arange(block, dtype=jnp.int32)
        key_pos = start - WINDOW + jnp.arange(reach, dtype=jnp.int32)
        allowed = (key_pos[None, :] >= 0) & (key_pos[None, :] < TOKENS)
        allowed = allowed & (jnp.abs(query_pos[:, None] - key_pos[None, :]) <= WINDOW)
        allowed = allowed & (query_docs[:, None] == key_docs[None, :])
        scores = jnp.einsum('qkgd,jkd->kgqj', query_blk.astype(jnp.float32), key_blk.astype(jnp.float32))
        scores = jnp.where(allowed, scores * HEAD_DIM ** (-0.5), masked_score)
        top_score = jnp.maximum(lax.optimization_barrier(jnp.max(scores, -1, keepdims=True)), sink_table)
        raised = jnp.where(allowed, jnp.exp(scores - top_score), 0.0)
        denominator = jnp.exp(sink_table - top_score) + lax.optimization_barrier(jnp.sum(raised, -1, keepdims=True))
        weights = (raised / denominator).astype(jnp.bfloat16)
        result = jnp.einsum('kgqj,jkd->qkgd', weights.astype(jnp.float32), value_blk.astype(jnp.float32))
        return result.astype(jnp.bfloat16).reshape(block, HEADS * HEAD_DIM)
    blocks = lax.map(one_block, jnp.arange(nblocks, dtype=jnp.int32))
    return blocks.reshape(TOKENS, HEADS * HEAD_DIM)

def experts_part(normed, route_ids, route_weights, expert_gate, expert_up, expert_down):
    nblocks = TOKENS // TOK_SUB
    slot_count = nblocks * CAP
    flat_ids = route_ids.reshape(nblocks, TOK_SUB * TOPK).astype(jnp.int32)
    one_hot = (flat_ids[:, :, None] == jnp.arange(EXPERTS, dtype=jnp.int32)[None, None, :]).astype(jnp.int32)
    ranks = (jnp.cumsum(one_hot, axis=1) - 1).astype(jnp.int32)
    slot_rank = lax.optimization_barrier(jnp.sum(ranks * one_hot, axis=-1)).astype(jnp.int32)
    block_ids = jnp.arange(nblocks, dtype=jnp.int32)[:, None]
    targets = (flat_ids * slot_count + block_ids * CAP + slot_rank).reshape(-1).astype(jnp.int32)
    owners = (block_ids * TOK_SUB + jnp.arange(TOK_SUB * TOPK, dtype=jnp.int32)[None, :] // TOPK).reshape(-1).astype(jnp.int32)
    token_table = jnp.full((EXPERTS * slot_count,), TOKENS, jnp.int32).at[targets].set(owners).reshape(EXPERTS, slot_count)
    weight_table = jnp.zeros((EXPERTS * slot_count,), jnp.float32).at[targets].set(route_weights.reshape(-1).astype(jnp.float32)).reshape(EXPERTS, slot_count)
    padded = jnp.concatenate([normed, jnp.zeros((1, D), normed.dtype)], 0)
    hidden_cols = FF // N_TP

    def one_expert(total, inputs):
        gate_weight, up_weight, down_weight, token_rows, row_weights = inputs
        row_block = jnp.take(padded, token_rows, axis=0)
        gate_act = jnp.dot(row_block, gate_weight, preferred_element_type=jnp.float32)
        up_act = jnp.dot(row_block, up_weight, preferred_element_type=jnp.float32)
        hidden = (jax.nn.silu(gate_act) * up_act).astype(jnp.bfloat16)
        summed = jnp.zeros((slot_count, D), jnp.float32)
        for member in range(N_TP):
            piece_out = jnp.dot(hidden[:, member * hidden_cols:(member + 1) * hidden_cols], down_weight[member * hidden_cols:(member + 1) * hidden_cols], preferred_element_type=jnp.float32)
            summed = summed + lax.optimization_barrier(piece_out.astype(jnp.bfloat16)).astype(jnp.float32)
        expert_out = lax.optimization_barrier(summed.astype(jnp.bfloat16)).astype(jnp.float32)
        return (total.at[token_rows].add(row_weights[:, None] * expert_out), None)
    total, _ = lax.scan(one_expert, jnp.zeros((TOKENS + 1, D), jnp.float32), (expert_gate, expert_up, expert_down, token_table, weight_table))
    return total[:TOKENS]

def reference(resid, queries, keys, values, doc_ids, sink_logits, out_proj, norm1_gain, norm1_bias, route_ids, route_weights, expert_gate, expert_up, expert_down, norm2_gain, norm2_bias):
    attended = attention(queries, keys, values, doc_ids, sink_logits)
    head_cols = ATT_WIDTH // N_TP
    projected = jnp.zeros((TOKENS, D), jnp.float32)
    for member in range(N_TP):
        piece_out = jnp.dot(attended[:, member * head_cols:(member + 1) * head_cols], out_proj[member * head_cols:(member + 1) * head_cols], preferred_element_type=jnp.float32)
        projected = projected + lax.optimization_barrier(piece_out.astype(jnp.bfloat16)).astype(jnp.float32)
    projected = lax.optimization_barrier(projected.astype(jnp.bfloat16)).astype(jnp.float32)
    pre_norm = residual_scale * resid.astype(jnp.float32) + projected
    normed = layer_norm(pre_norm, norm1_gain, norm1_bias).astype(jnp.bfloat16)
    moe_sum = experts_part(normed, route_ids, route_weights, expert_gate, expert_up, expert_down)
    pre_final = residual_scale * normed.astype(jnp.float32) + moe_sum
    return layer_norm(pre_final, norm2_gain, norm2_bias).astype(jnp.bfloat16)
```

```python
import functools

import jax
import jax.numpy as jnp
from jax import lax
from jax.experimental import pallas as pl
from jax.experimental.pallas import tpu as pltpu
from jax.sharding import PartitionSpec as P

HEAD_DIM = 64
WINDOW = 128
LANES = 128
GROUPS = 4
EPS = 1e-05
ROOT2 = 1.4142135623730951
MASKED = -1e30
MESH = pl.DeviceIdType.MESH
F32 = jnp.float32
BF16 = jnp.bfloat16


def offsets_far_first(nz):
    order = [nz // 2]
    for d in range(nz // 2 - 1, 0, -1):
        order += [d, -d]
    return order + [0]


def remote(src, dst, send_sem, recv_sem, device):
    return pltpu.make_async_remote_copy(
        src_ref=src, dst_ref=dst, send_sem=send_sem, recv_sem=recv_sem,
        device_id=device, device_id_type=MESH,
    )


def layer_norm(cells, gain, bias):
    mean = jnp.mean(cells, -1, keepdims=True)
    centred = cells - mean
    variance = jnp.mean(centred * centred, -1, keepdims=True)
    return centred * lax.rsqrt(variance + EPS) * gain + bias


def kernel(
    n_sp, cap,
    resid, queries, keys, values, docs, sinks, out_proj_hbm, gain1, bias1,
    route_ids, route_weights, gate_hbm, up_hbm, down_hbm, gain2, bias2,
    out,
    gate, up, down, out_proj, kk, vv, doc_own, doc_halo, attended,
    proj_part, proj_in, proj_left, proj_right, normed,
    wide, table, arrived, rows, hidden, part, sum_in, from_left, from_right,
    result, returned, acc,
    load_sems, halo_send, halo_recv, proj_send, proj_recv,
    z_send, z_recv, ag_send, ag_recv, rs_send, rs_recv, back_send, back_recv,
):
    sp = lax.axis_index("sp")
    tp = lax.axis_index("tp")
    n_tp = 4
    nz = n_sp // 2
    z, core = sp // 2, sp % 2
    right, left = (tp + 1) % n_tp, (tp + n_tp - 1) % n_tp
    to_right, to_left = {"tp": right}, {"tp": left}
    ahead, behind = (sp + 1) % n_sp, (sp + n_sp - 1) % n_sp
    tok_dev = queries.shape[0]
    tok_sub, width = resid.shape
    cut = width // LANES
    unit = cap * cut
    own_pad = kk.shape[0] - 2 * WINDOW
    order = offsets_far_first(nz)
    per_group = nz // GROUPS
    slots = 2 * per_group
    half = slots // 2 * unit
    whole = slots * unit
    n_rows = n_tp * slots * cap

    loads = [
        pltpu.make_async_copy(out_proj_hbm, out_proj, load_sems.at[0]),
        pltpu.make_async_copy(gate_hbm.at[0], gate, load_sems.at[1]),
        pltpu.make_async_copy(up_hbm.at[0], up, load_sems.at[2]),
        pltpu.make_async_copy(down_hbm.at[0], down, load_sems.at[3]),
    ]

    barrier = pltpu.get_barrier_semaphore()

    def greet(i, carry):
        pl.semaphore_signal(barrier, inc=1, device_id={"sp": (sp + i) % n_sp}, device_id_type=MESH)
        return carry

    lax.fori_loop(1, n_sp, greet, 0)
    pl.semaphore_signal(barrier, inc=1, device_id=to_right, device_id_type=MESH)
    pl.semaphore_signal(barrier, inc=1, device_id=to_left, device_id_type=MESH)
    for load in loads:
        load.start()

    k_own, v_own = keys[...], values[...]
    kk[pl.ds(0, tok_dev), :] = jnp.concatenate([k_own, k_own], axis=1)
    vv[pl.ds(0, tok_dev), :] = jnp.concatenate([v_own, v_own], axis=1)
    if own_pad > tok_dev:
        pad = jnp.zeros((own_pad - tok_dev, LANES), BF16)
        kk[pl.ds(tok_dev, own_pad - tok_dev), :] = pad
        vv[pl.ds(tok_dev, own_pad - tok_dev), :] = pad
    doc_own[...] = jnp.broadcast_to(docs[...], doc_own.shape)

    pl.semaphore_wait(barrier, n_sp + 1)

    tail = pl.ds(tok_dev - WINDOW, WINDOW)
    head = pl.ds(0, WINDOW)
    prev_slot, next_slot = pl.ds(own_pad, WINDOW), pl.ds(own_pad + WINDOW, WINDOW)
    halos = []
    for i, (src, dst, peer) in enumerate([
        (kk.at[tail], kk.at[prev_slot], ahead),
        (kk.at[head], kk.at[next_slot], behind),
        (doc_own, doc_halo.at[0], ahead),
        (doc_own, doc_halo.at[1], behind),
        (vv.at[tail], vv.at[prev_slot], ahead),
        (vv.at[head], vv.at[next_slot], behind),
    ]):
        copy = remote(src, dst, halo_send.at[i], halo_recv.at[i], {"sp": peer})
        copy.start()
        halos.append(copy)

    ids = route_ids[...].astype(F32)
    sub_i = lax.broadcasted_iota(jnp.int32, (tok_sub, tok_sub), 0)
    lane_i = lax.broadcasted_iota(jnp.int32, (tok_sub, tok_sub), 1)
    id_col = [ids[:, k : k + 1] for k in range(2)]
    id_row = [
        jnp.sum(jnp.where(sub_i == lane_i, c, 0.0), axis=0, keepdims=True) for c in id_col
    ]
    slot_row, slot_col = [], []
    for k in range(2):
        row, col = cap * id_row[k], cap * id_col[k]
        for other in range(2):
            same_row = (id_col[other] == id_row[k]) & (sub_i < lane_i)
            row = row + jnp.sum(jnp.where(same_row, 1.0, 0.0), axis=0, keepdims=True)
            same_col = (id_col[k] == id_row[other]) & (lane_i < sub_i)
            col = col + jnp.sum(jnp.where(same_col, 1.0, 0.0), axis=1, keepdims=True)
        slot_row.append(row)
        slot_col.append(col)
    n_slots = n_sp * cap
    slot_sub = lax.broadcasted_iota(jnp.int32, (n_slots, tok_sub), 0).astype(F32)
    slot_lane = lax.broadcasted_iota(jnp.int32, (tok_sub, n_slots), 1).astype(F32)
    assign = jnp.where(
        (slot_sub == slot_row[0]) | (slot_sub == slot_row[1]), 1.0, 0.0
    ).astype(BF16)
    choose = [jnp.where(slot_lane == c, 1.0, 0.0).astype(BF16) for c in slot_col]

    reach = own_pad + 2 * WINDOW
    for copy in halos[:4]:
        copy.wait_recv()
    doc_prev = doc_halo[0][0:1, :][:, tok_dev - WINDOW : tok_dev].astype(F32)
    doc_next = doc_halo[1][0:1, :][:, 0:WINDOW].astype(F32)
    doc_here = doc_own[0:1, :].astype(F32)
    if own_pad > tok_dev:
        doc_here = jnp.concatenate([doc_here, jnp.full((1, own_pad - tok_dev), -1.0, F32)], axis=1)
    doc_keys = jnp.concatenate([doc_here, doc_prev, doc_next], axis=1)
    q_sub = lax.broadcasted_iota(jnp.int32, (tok_dev, tok_dev), 0)
    q_lane = lax.broadcasted_iota(jnp.int32, (tok_dev, tok_dev), 1)
    doc_col = jnp.sum(
        jnp.where(q_sub == q_lane, doc_own[0:1, :].astype(F32), 0.0), axis=1, keepdims=True
    )
    lane = lax.broadcasted_iota(jnp.int32, (tok_dev, reach), 1)
    query = lax.broadcasted_iota(jnp.int32, (tok_dev, reach), 0)
    place = jnp.where(
        lane < own_pad, lane,
        jnp.where(lane < own_pad + WINDOW, lane - (own_pad + WINDOW), lane - (own_pad + WINDOW) + tok_dev),
    )
    at = place + sp * tok_dev
    allowed = (at >= 0) & (at < n_sp * tok_dev) & (jnp.abs(query - place) <= WINDOW)
    allowed = allowed & (doc_col == doc_keys)
    for copy in halos[4:]:
        copy.wait_recv()
    pair_lane = lax.broadcasted_iota(jnp.int32, (tok_dev, LANES), 1)
    for pair in range(queries.shape[1] // LANES):
        q_pair = queries[:, pair * LANES : (pair + 1) * LANES]
        outs = []
        for side in range(2):
            mine = (pair_lane < HEAD_DIM) if side == 0 else (pair_lane >= HEAD_DIM)
            q = jnp.where(mine, q_pair.astype(F32) * HEAD_DIM ** (-0.5), 0.0).astype(BF16)
            scores = lax.dot_general(
                q, kk[...], (((1,), (1,)), ((), ())), preferred_element_type=F32
            )
            scores = jnp.where(allowed, scores, MASKED)
            sink = sinks[2 * pair + side]
            top = jnp.maximum(jnp.max(scores, -1, keepdims=True), sink)
            raised = jnp.exp(scores - top)
            total = jnp.exp(sink - top) + jnp.sum(raised, -1, keepdims=True)
            weights = (raised * (1.0 / total)).astype(BF16)
            outs.append(jnp.dot(weights, vv[...], preferred_element_type=F32))
        attended[:, pair * LANES : (pair + 1) * LANES] = jnp.where(
            pair_lane < HEAD_DIM, outs[0], outs[1]
        ).astype(BF16)

    loads[0].wait()
    wide_half = width // 2
    opposite = (tp + 2) % n_tp

    def project(owner, j, h):
        block = attended[pl.ds(pl.multiple_of(owner * tok_sub, tok_sub), tok_sub), :]
        proj_part[j, h] = jnp.dot(
            block, out_proj[:, h * wide_half : (h + 1) * wide_half], preferred_element_type=F32
        ).astype(BF16)

    project(opposite, 3, 0)
    project(opposite, 3, 1)
    c_opp0 = remote(proj_part.at[3, 0], proj_in.at[0], proj_send.at[0], proj_recv.at[0], to_right)
    c_opp0.start()
    c_opp1 = remote(proj_part.at[3, 1], proj_in.at[1], proj_send.at[1], proj_recv.at[1], to_left)
    c_opp1.start()
    project(right, 2, 1)
    project(left, 1, 0)
    c_right1 = remote(proj_part.at[2, 1], proj_left.at[1], proj_send.at[2], proj_recv.at[2], to_right)
    c_right1.start()
    c_left0 = remote(proj_part.at[1, 0], proj_right.at[0], proj_send.at[3], proj_recv.at[3], to_left)
    c_left0.start()
    project(right, 2, 0)
    project(left, 1, 1)
    c_opp0.wait_recv()
    proj_part[2, 0] = (proj_part[2, 0].astype(F32) + proj_in[0].astype(F32)).astype(BF16)
    c_right0 = remote(proj_part.at[2, 0], proj_left.at[0], proj_send.at[4], proj_recv.at[4], to_right)
    c_right0.start()
    c_opp1.wait_recv()
    proj_part[1, 1] = (proj_part[1, 1].astype(F32) + proj_in[1].astype(F32)).astype(BF16)
    c_left1 = remote(proj_part.at[1, 1], proj_right.at[1], proj_send.at[5], proj_recv.at[5], to_left)
    c_left1.start()
    project(tp, 0, 0)
    project(tp, 0, 1)
    for copy in (c_right1, c_left0, c_right0, c_left1):
        copy.wait_recv()
    for h in range(2):
        cols = slice(h * wide_half, (h + 1) * wide_half)
        projected = (
            proj_part[0, h].astype(F32) + proj_left[h].astype(F32) + proj_right[h].astype(F32)
        ).astype(BF16)
        acc[:, cols] = ROOT2 * resid[:, cols].astype(F32) + projected.astype(F32)
    normed[...] = layer_norm(acc[...], gain1[...], bias1[...]).astype(BF16)

    for c in range(0, cut, 2):
        picked = jnp.dot(
            assign, normed[:, c * LANES : (c + 2) * LANES], preferred_element_type=F32
        )
        wide[pl.ds(c, n_slots, stride=cut), :] = picked[:, :LANES]
        wide[pl.ds(c + 1, n_slots, stride=cut), :] = picked[:, LANES:]
    for e in range(n_sp):
        table[e] = wide[pl.ds(e * unit, unit), :].astype(BF16)

    def place_of(g, i):
        return pl.ds((2 * i) * unit, unit), pl.ds((2 * i + 1) * unit, unit)

    for g in range(GROUPS):
        for i in range(per_group):
            o = order[g * per_group + i]
            if o == 0:
                dst = arrived.at[g, 0, pl.ds(2 * i * unit, unit)]
                partner = 2 * z + 1 - core
                remote(table.at[partner], dst, z_send.at[g], z_recv.at[g], {"sp": partner}).start()
            else:
                zd = (z + o + nz) % nz
                at_slot = pl.multiple_of((2 * i + core) * unit, unit)
                for cd in range(2):
                    e = 2 * zd + cd
                    dst = arrived.at[g, 0, pl.ds(at_slot, unit)]
                    remote(table.at[e], dst, z_send.at[g], z_recv.at[g], {"sp": e}).start()

    first, second = pl.ds(0, half), pl.ds(half, half)
    remote_z = [whole] * (GROUPS - 1) + [whole - unit]

    def z_done(g):
        region = arrived.at[g, 0, pl.ds(0, remote_z[g])]
        return remote(region, region, z_send.at[g], z_recv.at[g], to_right)

    ag_copies, rs_copies = [], []

    def ag(i, g, src, dst, device):
        copy = remote(src, dst, ag_send.at[i, g], ag_recv.at[i, g], device)
        ag_copies.append(copy)
        return copy

    def rs(i, g, src, dst, device):
        copy = remote(src, dst, rs_send.at[i, g], rs_recv.at[i, g], device)
        rs_copies.append(copy)
        return copy

    out_of = {}

    def step1(g):
        z_done(g).wait_recv()
        if g == GROUPS - 1:
            arrived[g, 0, pl.ds(whole - unit, unit), :] = table[sp]
        a = ag(0, g, arrived.at[g, 0], arrived.at[g, 1], to_right)
        a.start()
        b = ag(1, g, arrived.at[g, 0], arrived.at[g, 2], to_left)
        b.start()
        out_of["one", g] = (a, b)

    def step2(g):
        a, b = out_of["one", g]
        a.wait_recv()
        c = ag(2, g, arrived.at[g, 1, first], arrived.at[g, 3, first], to_right)
        c.start()
        b.wait_recv()
        d = ag(3, g, arrived.at[g, 2, second], arrived.at[g, 3, second], to_left)
        d.start()
        out_of["two", g] = (c, d)

    def step3(g):
        for copy in out_of["two", g]:
            copy.wait_recv()
        for j in range(n_tp):
            wide[pl.ds(j * whole, whole), :] = arrived[g, j].astype(F32)
        for c in range(cut):
            rows[:, c * LANES : (c + 1) * LANES] = wide[pl.ds(c, n_rows, stride=cut), :].astype(BF16)
        if g == 0:
            loads[1].wait()
            loads[2].wait()
            loads[3].wait()
        step = min(256, hidden.shape[1])

        def act(n, carry):
            cols = pl.ds(pl.multiple_of(n * step, step), step)
            a = jnp.dot(rows[...], gate[:, cols], preferred_element_type=F32)
            b = jnp.dot(rows[...], up[:, cols], preferred_element_type=F32)
            hidden[:, cols] = (a / (1.0 + jnp.exp(-a)) * b).astype(BF16)
            return carry

        lax.fori_loop(0, hidden.shape[1] // step, act, 0)
        for n in range(cut // 2):
            y = jnp.dot(
                hidden[...], down[:, n * 256 : (n + 1) * 256], preferred_element_type=F32
            )
            wide[pl.ds(2 * n, n_rows, stride=cut), :] = y[:, :LANES]
            wide[pl.ds(2 * n + 1, n_rows, stride=cut), :] = y[:, LANES:]
        for j in (3, 1, 2, 0):
            part[g, j] = wide[pl.ds(j * whole, whole), :].astype(BF16)
        a = rs(0, g, part.at[g, 3, first], sum_in.at[g, 0], to_right)
        b = rs(1, g, part.at[g, 3, second], sum_in.at[g, 1], to_left)
        c = rs(2, g, part.at[g, 2, second], from_left.at[g, second], to_right)
        d = rs(3, g, part.at[g, 1, first], from_right.at[g, first], to_left)
        for copy in (a, b, c, d):
            copy.start()
        out_of["three", g] = (a, b, c, d)

    def step4(g):
        a, b, c, d = out_of["three", g]
        a.wait_recv()
        part[g, 2, first, :] = (part[g, 2, first, :].astype(F32) + sum_in[g, 0].astype(F32)).astype(BF16)
        e = rs(4, g, part.at[g, 2, first], from_left.at[g, first], to_right)
        e.start()
        b.wait_recv()
        part[g, 1, second, :] = (part[g, 1, second, :].astype(F32) + sum_in[g, 1].astype(F32)).astype(BF16)
        f = rs(5, g, part.at[g, 1, second], from_right.at[g, second], to_left)
        f.start()
        out_of["four", g] = (c, d, e, f)

    def step5(g):
        for copy in out_of["four", g]:
            copy.wait_recv()
        result[g] = (
            part[g, 0].astype(F32) + from_left[g].astype(F32) + from_right[g].astype(F32)
        ).astype(BF16)
        for i in range(per_group):
            o = order[g * per_group + i]
            for cs in range(2):
                src = pl.ds((2 * i + cs) * unit, unit)
                if o == 0 and cs == 1:
                    returned[sp] = result[g, src, :]
                else:
                    peer = 2 * z + 1 - core if o == 0 else 2 * ((z - o + nz) % nz) + cs
                    remote(
                        result.at[g, src], returned.at[sp], back_send.at[g], back_recv.at[0], {"sp": peer}
                    ).start()

    step1(0)
    step2(0)
    step1(1)
    step3(0)
    step2(1)
    step4(0)
    step1(2)
    step3(1)
    step5(0)
    step2(2)
    step4(1)
    step1(3)
    step3(2)
    step5(1)
    step2(3)
    step4(2)
    step3(3)
    step5(2)
    step4(3)
    step5(3)

    region = returned.at[pl.ds(0, n_sp - 1)]
    remote(region, region, back_send.at[0], back_recv.at[0], to_right).wait_recv()
    for e in range(n_sp):
        wide[pl.ds(e * unit, unit), :] = returned[e].astype(F32)
    share = [route_weights[:, k : k + 1] for k in range(2)]
    for c in range(0, cut, 2):
        cols = slice(c * LANES, (c + 2) * LANES)
        cells = jnp.concatenate(
            [wide[pl.ds(c + i, n_slots, stride=cut), :].astype(BF16) for i in range(2)], axis=1
        )
        total = ROOT2 * normed[:, cols].astype(F32)
        moe = share[0] * jnp.dot(choose[0], cells, preferred_element_type=F32)
        moe = moe + share[1] * jnp.dot(choose[1], cells, preferred_element_type=F32)
        acc[:, cols] = total + moe
    out[...] = layer_norm(acc[...], gain2[...], bias2[...]).astype(BF16)

    for copy in halos:
        copy.wait_send()
    for copy in (c_opp0, c_opp1, c_right1, c_left0, c_right0, c_left1):
        copy.wait_send()
    for copy in ag_copies + rs_copies:
        copy.wait_send()
    for g in range(GROUPS):
        z_done(g).wait_send()
        region = result.at[g, pl.ds(0, remote_z[g])]
        remote(region, region, back_send.at[g], back_recv.at[0], to_right).wait_send()


def per_device(
    resid, queries, keys, values, doc_ids, sink_logits, out_proj, norm1_gain, norm1_bias,
    route_ids, route_weights, expert_gate, expert_up, expert_down, norm2_gain, norm2_bias,
):
    n_sp = lax.axis_size("sp")
    tok_dev, att = queries.shape
    tok_sub, width = resid.shape
    ff = expert_gate.shape[2]
    cap = 2 * tok_sub // n_sp
    cut = width // LANES
    unit = cap * cut
    own_pad = -(-tok_dev // LANES) * LANES
    slots = n_sp // GROUPS
    whole = slots * unit
    half = whole // 2
    n_rows = 4 * slots * cap
    vmem = pl.BlockSpec(memory_space=pltpu.VMEM)
    hbm = pl.BlockSpec(memory_space=pl.ANY)
    dma = pltpu.SemaphoreType.DMA
    scratch = [
        pltpu.VMEM((width, ff), BF16),
        pltpu.VMEM((width, ff), BF16),
        pltpu.VMEM((ff, width), BF16),
        pltpu.VMEM((att, width), BF16),
        pltpu.VMEM((own_pad + 2 * WINDOW, LANES), BF16),
        pltpu.VMEM((own_pad + 2 * WINDOW, LANES), BF16),
        pltpu.VMEM((8, tok_dev), jnp.int32),
        pltpu.VMEM((2, 8, tok_dev), jnp.int32),
        pltpu.VMEM((tok_dev, att), BF16),
        pltpu.VMEM((4, 2, tok_sub, width // 2), BF16),
        pltpu.VMEM((2, tok_sub, width // 2), BF16),
        pltpu.VMEM((2, tok_sub, width // 2), BF16),
        pltpu.VMEM((2, tok_sub, width // 2), BF16),
        pltpu.VMEM((tok_sub, width), BF16),
        pltpu.VMEM((max(n_sp * unit, 4 * whole), LANES), F32),
        pltpu.VMEM((n_sp, unit, LANES), BF16),
        pltpu.VMEM((GROUPS, 4, whole, LANES), BF16),
        pltpu.VMEM((n_rows, width), BF16),
        pltpu.VMEM((n_rows, ff), BF16),
        pltpu.VMEM((GROUPS, 4, whole, LANES), BF16),
        pltpu.VMEM((GROUPS, 2, half, LANES), BF16),
        pltpu.VMEM((GROUPS, whole, LANES), BF16),
        pltpu.VMEM((GROUPS, whole, LANES), BF16),
        pltpu.VMEM((GROUPS, whole, LANES), BF16),
        pltpu.VMEM((n_sp, unit, LANES), BF16),
        pltpu.VMEM((tok_sub, width), F32),
        dma((4,)), dma((6,)), dma((6,)), dma((6,)), dma((6,)),
        dma((GROUPS,)), dma((GROUPS,)), dma((4, GROUPS)), dma((4, GROUPS)),
        dma((6, GROUPS)), dma((6, GROUPS)), dma((GROUPS,)), dma((1,)),
    ]
    flops = 2 * tok_dev * att * width + 2 * 4 * tok_sub * 2 * width * ff * 3
    return pl.pallas_call(
        functools.partial(kernel, n_sp, cap),
        out_shape=jax.ShapeDtypeStruct((tok_sub, width), BF16),
        in_specs=[
            vmem, vmem, vmem, vmem, vmem, pl.BlockSpec(memory_space=pltpu.SMEM), hbm,
            vmem, vmem, vmem, vmem, hbm, hbm, hbm, vmem, vmem,
        ],
        out_specs=vmem,
        scratch_shapes=scratch,
        compiler_params=pltpu.CompilerParams(
            collective_id=0, has_side_effects=True, vmem_limit_bytes=56 * 1024 * 1024
        ),
        cost_estimate=pl.CostEstimate(flops=flops, bytes_accessed=12_000_000, transcendentals=0),
        name="layer",
    )(
        resid, queries, keys, values, doc_ids[None, :], sink_logits, out_proj,
        norm1_gain[None, :], norm1_bias[None, :], route_ids, route_weights,
        expert_gate, expert_up, expert_down, norm2_gain[None, :], norm2_bias[None, :],
    )


def solution(mesh):
    rows = ("grp", "sp", "tp")
    placed = (
        P(rows, None),
        P(("grp", "sp"), "tp"),
        P(("grp", "sp"), "tp"),
        P(("grp", "sp"), "tp"),
        P(("grp", "sp")),
        P("tp"),
        P("tp", None),
        P(),
        P(),
        P(rows, None),
        P(rows, None),
        P("sp", None, "tp"),
        P("sp", None, "tp"),
        P("sp", "tp", None),
        P(),
        P(),
    )
    return jax.shard_map(
        per_device, mesh=mesh, in_specs=placed, out_specs=P(rows, None), check_vma=False
    )
```

```python
import functools

import jax
import jax.numpy as jnp
from jax import lax
from jax.experimental import pallas as pl
from jax.experimental.pallas import tpu as pltpu
from jax.sharding import PartitionSpec as P

HEAD_DIM = 64
WINDOW = 128
LANES = 128
GROUPS = 4
EPS = 1e-05
ROOT2 = 1.4142135623730951
MASKED = -1e30
MESH = pl.DeviceIdType.MESH
F32 = jnp.float32
BF16 = jnp.bfloat16


def remote(src, dst, send_sem, recv_sem, device):
    return pltpu.make_async_remote_copy(
        src_ref=src, dst_ref=dst, send_sem=send_sem, recv_sem=recv_sem,
        device_id=device, device_id_type=MESH,
    )


def layer_norm(cells, gain, bias):
    mean = jnp.mean(cells, -1, keepdims=True)
    centred = cells - mean
    variance = jnp.mean(centred * centred, -1, keepdims=True)
    return centred * lax.rsqrt(variance + EPS) * gain + bias


def kernel(
    n_sp, cap,
    resid, queries, keys, values, docs, sinks, out_proj_hbm, gain1, bias1,
    route_ids, route_weights, gate_hbm, up_hbm, down_hbm, gain2, bias2,
    out,
    gate, up, down, out_proj, kk, vv, doc_own, doc_halo, attended,
    proj_part, proj_in, proj_left, proj_right, normed,
    wide, table, arrived, rows, hidden, part, sum_in, from_left, from_right,
    result, returned, acc,
    load_sems, halo_send, halo_recv, proj_send, proj_recv,
    chain, present, z_send, z_recv, ag_send, ag_recv, rs_send, rs_recv, back_send, back_recv,
):
    sp = lax.axis_index("sp")
    tp = lax.axis_index("tp")
    n_tp = 4
    core = sp % 2
    right, left = (tp + 1) % n_tp, (tp + n_tp - 1) % n_tp
    to_right, to_left = {"tp": right}, {"tp": left}
    last = n_sp - 1
    partner = sp + 1 - 2 * core
    across = sp - 1 + 2 * core
    has_across = (across >= 0) & (across <= last)
    tok_dev = queries.shape[0]
    tok_sub, width = resid.shape
    cut = width // LANES
    unit = cap * cut
    my_group, my_slot = sp // (n_sp // GROUPS), sp % (n_sp // GROUPS)
    own_pad = kk.shape[0] - 2 * WINDOW
    slots = n_sp // GROUPS
    half = slots // 2 * unit
    whole = slots * unit
    n_rows = n_tp * slots * cap

    loads = [
        pltpu.make_async_copy(out_proj_hbm, out_proj, load_sems.at[0]),
        pltpu.make_async_copy(gate_hbm.at[0], gate, load_sems.at[1]),
        pltpu.make_async_copy(up_hbm.at[0], up, load_sems.at[2]),
        pltpu.make_async_copy(down_hbm.at[0], down, load_sems.at[3]),
    ]

    barrier = pltpu.get_barrier_semaphore()

    def tell(sem, device):
        pl.semaphore_signal(sem, inc=1, device_id=device, device_id_type=MESH)

    tell(barrier, to_right)
    tell(barrier, to_left)
    tell(barrier, {"sp": partner})

    @pl.when(has_across)
    def _():
        tell(barrier, {"sp": across})

    for load in loads:
        load.start()

    def doubled(cells):
        return jnp.transpose(jnp.concatenate([cells, cells], axis=0).astype(F32)).astype(BF16)

    kk[pl.ds(0, tok_dev), :] = doubled(keys[...])
    vv[pl.ds(0, tok_dev), :] = doubled(values[...])
    if own_pad > tok_dev:
        pad = jnp.zeros((own_pad - tok_dev, LANES), BF16)
        kk[pl.ds(tok_dev, own_pad - tok_dev), :] = pad
        vv[pl.ds(tok_dev, own_pad - tok_dev), :] = pad
    doc_own[...] = jnp.broadcast_to(docs[...], doc_own.shape)

    prev_slot, next_slot = pl.ds(own_pad, WINDOW), pl.ds(own_pad + WINDOW, WINDOW)

    def blank(slot, i):
        kk[slot, :] = jnp.zeros((WINDOW, LANES), BF16)
        vv[slot, :] = jnp.zeros((WINDOW, LANES), BF16)
        doc_halo[i] = jnp.zeros(doc_own.shape, jnp.int32)

    @pl.when(sp == 0)
    def _():
        blank(prev_slot, 0)

    @pl.when(sp == last)
    def _():
        blank(next_slot, 1)

    pl.semaphore_wait(barrier, jnp.where(has_across, 4, 3))

    tail = pl.ds(tok_dev - WINDOW, WINDOW)
    head = pl.ds(0, WINDOW)
    to_next, to_prev = {"sp": (sp + 1) % n_sp}, {"sp": (sp + last) % n_sp}
    halos_up = [
        remote(src, dst, halo_send.at[i], halo_recv.at[i], to_next)
        for i, (src, dst) in enumerate([
            (doc_own, doc_halo.at[0]), (kk.at[tail], kk.at[prev_slot]), (vv.at[tail], vv.at[prev_slot]),
        ])
    ]
    halos_down = [
        remote(src, dst, halo_send.at[i], halo_recv.at[i], to_prev)
        for i, (src, dst) in enumerate([
            (doc_own, doc_halo.at[1]), (kk.at[head], kk.at[next_slot]), (vv.at[head], vv.at[next_slot]),
        ], 3)
    ]

    @pl.when(sp < last)
    def _():
        for copy in halos_up:
            copy.start()

    @pl.when(sp > 0)
    def _():
        for copy in halos_down:
            copy.start()

    @pl.when(sp > 0)
    def _():
        pl.semaphore_wait(chain, 1)

    @pl.when(sp < last)
    def _():
        tell(chain, to_next)

    def tell_below(d, carry):
        tell(present.at[sp], {"sp": d})
        return carry

    lax.fori_loop(0, sp, tell_below, 0)

    ids = route_ids[...].astype(F32)
    sub_i = lax.broadcasted_iota(jnp.int32, (tok_sub, tok_sub), 0)
    lane_i = lax.broadcasted_iota(jnp.int32, (tok_sub, tok_sub), 1)

    def upright(row):
        return jnp.sum(jnp.where(sub_i == lane_i, row, 0.0), axis=1, keepdims=True)

    id_row = [ids[k : k + 1, :] for k in range(2)]
    id_col = [upright(row) for row in id_row]
    share = [upright(route_weights[k : k + 1, :]) for k in range(2)]
    slot_row, slot_col = [], []
    for k in range(2):
        row, col = cap * id_row[k], cap * id_col[k]
        for other in range(2):
            same_row = (id_col[other] == id_row[k]) & (sub_i < lane_i)
            row = row + jnp.sum(jnp.where(same_row, 1.0, 0.0), axis=0, keepdims=True)
            same_col = (id_col[k] == id_row[other]) & (lane_i < sub_i)
            col = col + jnp.sum(jnp.where(same_col, 1.0, 0.0), axis=1, keepdims=True)
        slot_row.append(row)
        slot_col.append(col)
    n_slots = n_sp * cap
    slot_sub = lax.broadcasted_iota(jnp.int32, (n_slots, tok_sub), 0).astype(F32)
    slot_lane = lax.broadcasted_iota(jnp.int32, (tok_sub, n_slots), 1).astype(F32)
    assign = jnp.where(
        (slot_sub == slot_row[0]) | (slot_sub == slot_row[1]), 1.0, 0.0
    ).astype(BF16)
    choose = [jnp.where(slot_lane == c, 1.0, 0.0).astype(BF16) for c in slot_col]

    reach = own_pad + 2 * WINDOW
    @pl.when(sp > 0)
    def _():
        for copy in halos_up:
            copy.wait_recv()

    @pl.when(sp < last)
    def _():
        for copy in halos_down:
            copy.wait_recv()

    doc_prev = doc_halo[0][0:1, :][:, tok_dev - WINDOW : tok_dev].astype(F32)
    doc_next = doc_halo[1][0:1, :][:, 0:WINDOW].astype(F32)
    doc_here = doc_own[0:1, :].astype(F32)
    if own_pad > tok_dev:
        doc_here = jnp.concatenate([doc_here, jnp.full((1, own_pad - tok_dev), -1.0, F32)], axis=1)
    doc_keys = jnp.concatenate([doc_here, doc_prev, doc_next], axis=1)
    q_sub = lax.broadcasted_iota(jnp.int32, (tok_dev, tok_dev), 0)
    q_lane = lax.broadcasted_iota(jnp.int32, (tok_dev, tok_dev), 1)
    doc_col = jnp.sum(
        jnp.where(q_sub == q_lane, doc_own[0:1, :].astype(F32), 0.0), axis=1, keepdims=True
    )
    lane = lax.broadcasted_iota(jnp.int32, (tok_dev, reach), 1)
    query = lax.broadcasted_iota(jnp.int32, (tok_dev, reach), 0)
    place = jnp.where(
        lane < own_pad, lane,
        jnp.where(lane < own_pad + WINDOW, lane - (own_pad + WINDOW), lane - (own_pad + WINDOW) + tok_dev),
    )
    at = place + sp * tok_dev
    allowed = (at >= 0) & (at < n_sp * tok_dev) & (jnp.abs(query - place) <= WINDOW)
    allowed = allowed & (doc_col == doc_keys)
    pair_lane = lax.broadcasted_iota(jnp.int32, (tok_dev, LANES), 1)
    for pair in range(queries.shape[1] // LANES):
        q_pair = queries[:, pair * LANES : (pair + 1) * LANES]
        outs = []
        for side in range(2):
            mine = (pair_lane < HEAD_DIM) if side == 0 else (pair_lane >= HEAD_DIM)
            q = jnp.where(mine, q_pair.astype(F32) * HEAD_DIM ** (-0.5), 0.0).astype(BF16)
            scores = lax.dot_general(
                q, kk[...], (((1,), (1,)), ((), ())), preferred_element_type=F32
            )
            scores = jnp.where(allowed, scores, MASKED)
            sink = sinks[2 * pair + side]
            top = jnp.maximum(jnp.max(scores, -1, keepdims=True), sink)
            raised = jnp.exp(scores - top)
            total = jnp.exp(sink - top) + jnp.sum(raised, -1, keepdims=True)
            weights = (raised * (1.0 / total)).astype(BF16)
            outs.append(jnp.dot(weights, vv[...], preferred_element_type=F32))
        attended[:, pair * LANES : (pair + 1) * LANES] = jnp.where(
            pair_lane < HEAD_DIM, outs[0], outs[1]
        ).astype(BF16)

    loads[0].wait()
    wide_half = width // 2
    opposite = (tp + 2) % n_tp

    def project(owner, j, h):
        block = attended[pl.ds(pl.multiple_of(owner * tok_sub, tok_sub), tok_sub), :]
        proj_part[j, h] = jnp.dot(
            block, out_proj[:, h * wide_half : (h + 1) * wide_half], preferred_element_type=F32
        ).astype(BF16)

    project(opposite, 3, 0)
    project(opposite, 3, 1)
    c_opp0 = remote(proj_part.at[3, 0], proj_in.at[0], proj_send.at[0], proj_recv.at[0], to_right)
    c_opp0.start()
    c_opp1 = remote(proj_part.at[3, 1], proj_in.at[1], proj_send.at[1], proj_recv.at[1], to_left)
    c_opp1.start()
    project(right, 2, 1)
    project(left, 1, 0)
    c_right1 = remote(proj_part.at[2, 1], proj_left.at[1], proj_send.at[2], proj_recv.at[2], to_right)
    c_right1.start()
    c_left0 = remote(proj_part.at[1, 0], proj_right.at[0], proj_send.at[3], proj_recv.at[3], to_left)
    c_left0.start()
    project(right, 2, 0)
    project(left, 1, 1)
    c_opp0.wait_recv()
    proj_part[2, 0] = (proj_part[2, 0].astype(F32) + proj_in[0].astype(F32)).astype(BF16)
    c_right0 = remote(proj_part.at[2, 0], proj_left.at[0], proj_send.at[4], proj_recv.at[4], to_right)
    c_right0.start()
    c_opp1.wait_recv()
    proj_part[1, 1] = (proj_part[1, 1].astype(F32) + proj_in[1].astype(F32)).astype(BF16)
    c_left1 = remote(proj_part.at[1, 1], proj_right.at[1], proj_send.at[5], proj_recv.at[5], to_left)
    c_left1.start()
    project(tp, 0, 0)
    project(tp, 0, 1)
    for copy in (c_right1, c_left0, c_right0, c_left1):
        copy.wait_recv()
    for h in range(2):
        cols = slice(h * wide_half, (h + 1) * wide_half)
        projected = (
            proj_part[0, h].astype(F32) + proj_left[h].astype(F32) + proj_right[h].astype(F32)
        ).astype(BF16)
        acc[:, cols] = ROOT2 * resid[:, cols].astype(F32) + projected.astype(F32)
    normed[...] = layer_norm(acc[...], gain1[...], bias1[...]).astype(BF16)

    for c in range(0, cut, 2):
        picked = jnp.dot(
            assign, normed[:, c * LANES : (c + 2) * LANES], preferred_element_type=F32
        )
        wide[pl.ds(c, n_slots, stride=cut), :] = picked[:, :LANES]
        wide[pl.ds(c + 1, n_slots, stride=cut), :] = picked[:, LANES:]
    for e in range(n_sp):
        table[e] = wide[pl.ds(e * unit, unit), :].astype(BF16)
    my_place = pl.ds(pl.multiple_of(my_slot * unit, unit), unit)
    arrived[my_group, 0, my_place, :] = table[sp]

    def dispatch(d):
        remote(
            table.at[d], arrived.at[my_group, 0, my_place], z_send.at[0], z_recv.at[sp], {"sp": d}
        ).start()

    def dispatch_down(i, carry):
        dispatch(sp - i)
        return carry

    def dispatch_up(d, carry):
        pl.semaphore_wait(present.at[d], 1)
        dispatch(d)
        return carry

    lax.fori_loop(1, sp + 1, dispatch_down, 0)
    lax.fori_loop(sp + 1, n_sp, dispatch_up, 0)

    first, second = pl.ds(0, half), pl.ds(half, half)
    ag_copies, rs_copies = [], []

    def ag(i, g, src, dst, device):
        copy = remote(src, dst, ag_send.at[i, g], ag_recv.at[i, g], device)
        ag_copies.append(copy)
        return copy

    def rs(i, g, src, dst, device):
        copy = remote(src, dst, rs_send.at[i, g], rs_recv.at[i, g], device)
        rs_copies.append(copy)
        return copy

    out_of = {}

    def step1(g):
        for i in range(slots):
            s = g * slots + i
            place = arrived.at[g, 0, pl.ds(i * unit, unit)]

            @pl.when(s != sp)
            def _():
                remote(place, place, z_send.at[0], z_recv.at[s], to_right).wait_recv()

        a = ag(0, g, arrived.at[g, 0], arrived.at[g, 1], to_right)
        a.start()
        b = ag(1, g, arrived.at[g, 0], arrived.at[g, 2], to_left)
        b.start()
        out_of["one", g] = (a, b)

    def step2(g):
        a, b = out_of["one", g]
        a.wait_recv()
        c = ag(2, g, arrived.at[g, 1, first], arrived.at[g, 3, first], to_right)
        c.start()
        b.wait_recv()
        d = ag(3, g, arrived.at[g, 2, second], arrived.at[g, 3, second], to_left)
        d.start()
        out_of["two", g] = (c, d)

    def step3(g):
        for copy in out_of["two", g]:
            copy.wait_recv()
        for j in range(n_tp):
            wide[pl.ds(j * whole, whole), :] = arrived[g, j].astype(F32)
        for c in range(cut):
            rows[:, c * LANES : (c + 1) * LANES] = wide[pl.ds(c, n_rows, stride=cut), :].astype(BF16)
        if g == 0:
            loads[1].wait()
            loads[2].wait()
            loads[3].wait()
        step = min(256, hidden.shape[1])

        def act(n, carry):
            cols = pl.ds(pl.multiple_of(n * step, step), step)
            a = jnp.dot(rows[...], gate[:, cols], preferred_element_type=F32)
            b = jnp.dot(rows[...], up[:, cols], preferred_element_type=F32)
            hidden[:, cols] = (a / (1.0 + jnp.exp(-a)) * b).astype(BF16)
            return carry

        lax.fori_loop(0, hidden.shape[1] // step, act, 0)
        for n in range(cut // 2):
            y = jnp.dot(
                hidden[...], down[:, n * 256 : (n + 1) * 256], preferred_element_type=F32
            )
            wide[pl.ds(2 * n, n_rows, stride=cut), :] = y[:, :LANES]
            wide[pl.ds(2 * n + 1, n_rows, stride=cut), :] = y[:, LANES:]
        for j in (3, 1, 2, 0):
            part[g, j] = wide[pl.ds(j * whole, whole), :].astype(BF16)
        a = rs(0, g, part.at[g, 3, first], sum_in.at[g, 0], to_right)
        b = rs(1, g, part.at[g, 3, second], sum_in.at[g, 1], to_left)
        c = rs(2, g, part.at[g, 2, second], from_left.at[g, second], to_right)
        d = rs(3, g, part.at[g, 1, first], from_right.at[g, first], to_left)
        for copy in (a, b, c, d):
            copy.start()
        out_of["three", g] = (a, b, c, d)

    def step4(g):
        a, b, c, d = out_of["three", g]
        a.wait_recv()
        part[g, 2, first, :] = (part[g, 2, first, :].astype(F32) + sum_in[g, 0].astype(F32)).astype(BF16)
        e = rs(4, g, part.at[g, 2, first], from_left.at[g, first], to_right)
        e.start()
        b.wait_recv()
        part[g, 1, second, :] = (part[g, 1, second, :].astype(F32) + sum_in[g, 1].astype(F32)).astype(BF16)
        f = rs(5, g, part.at[g, 1, second], from_right.at[g, second], to_left)
        f.start()
        out_of["four", g] = (c, d, e, f)

    def step5(g):
        for copy in out_of["four", g]:
            copy.wait_recv()
        result[g] = (
            part[g, 0].astype(F32) + from_left[g].astype(F32) + from_right[g].astype(F32)
        ).astype(BF16)
        for i in range(slots):
            s = g * slots + i
            src = pl.ds(i * unit, unit)

            @pl.when(s != sp)
            def _():
                remote(
                    result.at[g, src], returned.at[sp], back_send.at[0], back_recv.at[0], {"sp": s}
                ).start()

            @pl.when(s == sp)
            def _():
                returned[sp] = result[g, src, :]

    step1(0)
    step2(0)
    step1(1)
    step3(0)
    step2(1)
    step1(2)
    step4(0)
    step3(1)
    step2(2)
    step5(0)
    step4(1)
    step1(3)
    step3(2)
    step5(1)
    step2(3)
    step4(2)
    step3(3)
    step5(2)
    step4(3)
    step5(3)

    others = returned.at[pl.ds(0, last)]
    remote(others, others, back_send.at[0], back_recv.at[0], to_right).wait_recv()
    for e in range(n_sp):
        wide[pl.ds(e * unit, unit), :] = returned[e].astype(F32)
    for c in range(0, cut, 2):
        cols = slice(c * LANES, (c + 2) * LANES)
        cells = jnp.concatenate(
            [wide[pl.ds(c + i, n_slots, stride=cut), :].astype(BF16) for i in range(2)], axis=1
        )
        total = ROOT2 * normed[:, cols].astype(F32)
        moe = share[0] * jnp.dot(choose[0], cells, preferred_element_type=F32)
        moe = moe + share[1] * jnp.dot(choose[1], cells, preferred_element_type=F32)
        acc[:, cols] = total + moe
    out[...] = layer_norm(acc[...], gain2[...], bias2[...]).astype(BF16)

    @pl.when(sp < last)
    def _():
        for copy in halos_up:
            copy.wait_send()

    @pl.when(sp > 0)
    def _():
        for copy in halos_down:
            copy.wait_send()

    for copy in (c_opp0, c_opp1, c_right1, c_left0, c_right0, c_left1):
        copy.wait_send()
    for copy in ag_copies + rs_copies:
        copy.wait_send()
    remote(others, others, z_send.at[0], z_recv.at[0], to_right).wait_send()
    remote(others, others, back_send.at[0], back_recv.at[0], to_right).wait_send()


def per_device(
    resid, queries, keys, values, doc_ids, sink_logits, out_proj, norm1_gain, norm1_bias,
    route_ids, route_weights, expert_gate, expert_up, expert_down, norm2_gain, norm2_bias,
):
    n_sp = lax.axis_size("sp")
    tok_dev, att = queries.shape
    tok_sub, width = resid.shape
    ff = expert_gate.shape[2]
    cap = 2 * tok_sub // n_sp
    cut = width // LANES
    unit = cap * cut
    own_pad = -(-tok_dev // LANES) * LANES
    slots = n_sp // GROUPS
    whole = slots * unit
    half = whole // 2
    n_rows = 4 * slots * cap
    vmem = pl.BlockSpec(memory_space=pltpu.VMEM)
    hbm = pl.BlockSpec(memory_space=pl.ANY)
    dma = pltpu.SemaphoreType.DMA
    scratch = [
        pltpu.VMEM((width, ff), BF16),
        pltpu.VMEM((width, ff), BF16),
        pltpu.VMEM((ff, width), BF16),
        pltpu.VMEM((att, width), BF16),
        pltpu.VMEM((own_pad + 2 * WINDOW, LANES), BF16),
        pltpu.VMEM((own_pad + 2 * WINDOW, LANES), BF16),
        pltpu.VMEM((8, tok_dev), jnp.int32),
        pltpu.VMEM((2, 8, tok_dev), jnp.int32),
        pltpu.VMEM((tok_dev, att), BF16),
        pltpu.VMEM((4, 2, tok_sub, width // 2), BF16),
        pltpu.VMEM((2, tok_sub, width // 2), BF16),
        pltpu.VMEM((2, tok_sub, width // 2), BF16),
        pltpu.VMEM((2, tok_sub, width // 2), BF16),
        pltpu.VMEM((tok_sub, width), BF16),
        pltpu.VMEM((max(n_sp * unit, 4 * whole), LANES), F32),
        pltpu.VMEM((n_sp, unit, LANES), BF16),
        pltpu.VMEM((GROUPS, 4, whole, LANES), BF16),
        pltpu.VMEM((n_rows, width), BF16),
        pltpu.VMEM((n_rows, ff), BF16),
        pltpu.VMEM((GROUPS, 4, whole, LANES), BF16),
        pltpu.VMEM((GROUPS, 2, half, LANES), BF16),
        pltpu.VMEM((GROUPS, whole, LANES), BF16),
        pltpu.VMEM((GROUPS, whole, LANES), BF16),
        pltpu.VMEM((GROUPS, whole, LANES), BF16),
        pltpu.VMEM((n_sp, unit, LANES), BF16),
        pltpu.VMEM((tok_sub, width), F32),
        dma((4,)), dma((6,)), dma((6,)), dma((6,)), dma((6,)),
        pltpu.SemaphoreType.REGULAR, pltpu.SemaphoreType.REGULAR((n_sp,)),
        dma((1,)), dma((n_sp,)), dma((4, GROUPS)), dma((4, GROUPS)),
        dma((6, GROUPS)), dma((6, GROUPS)), dma((1,)), dma((1,)),
    ]
    flops = 2 * tok_dev * att * width + 2 * 4 * tok_sub * 2 * width * ff * 3
    return pl.pallas_call(
        functools.partial(kernel, n_sp, cap),
        out_shape=jax.ShapeDtypeStruct((tok_sub, width), BF16),
        in_specs=[
            vmem, vmem, vmem, vmem, vmem, pl.BlockSpec(memory_space=pltpu.SMEM), hbm,
            vmem, vmem, vmem, vmem, hbm, hbm, hbm, vmem, vmem,
        ],
        out_specs=vmem,
        scratch_shapes=scratch,
        compiler_params=pltpu.CompilerParams(
            collective_id=0, has_side_effects=True, vmem_limit_bytes=56 * 1024 * 1024
        ),
        cost_estimate=pl.CostEstimate(flops=flops, bytes_accessed=12_000_000, transcendentals=0),
        name="layer",
    )(
        resid, queries, keys.T, values.T, doc_ids[None, :], sink_logits, out_proj,
        norm1_gain[None, :], norm1_bias[None, :], route_ids.T, route_weights.T,
        expert_gate, expert_up, expert_down, norm2_gain[None, :], norm2_bias[None, :],
    )


def solution(mesh):
    rows = ("grp", "sp", "tp")
    placed = (
        P(rows, None),
        P(("grp", "sp"), "tp"),
        P(("grp", "sp"), "tp"),
        P(("grp", "sp"), "tp"),
        P(("grp", "sp")),
        P("tp"),
        P("tp", None),
        P(),
        P(),
        P(rows, None),
        P(rows, None),
        P("sp", None, "tp"),
        P("sp", None, "tp"),
        P("sp", "tp", None),
        P(),
        P(),
    )
    return jax.shard_map(
        per_device, mesh=mesh, in_specs=placed, out_specs=P(rows, None), check_vma=False
    )
```

```python
import functools

import jax
import jax.numpy as jnp
from jax import lax
from jax.experimental import pallas as pl
from jax.experimental.pallas import tpu as pltpu
from jax.sharding import PartitionSpec as P

HEAD_DIM = 64
WINDOW = 128
LANES = 128
EPS = 1e-05
ROOT2 = 1.4142135623730951
MASKED = -1e30
MESH = pl.DeviceIdType.MESH
F32 = jnp.float32
BF16 = jnp.bfloat16


def groups_of(nz):
    base, extra = nz // 4, nz // 16
    edges = (0, base + extra, 2 * base + extra, 3 * base + extra, nz)
    return tuple(zip(edges[:-1], edges[1:]))


def offset_of(i):
    return (i + 1) // 2 if i % 2 else -(i // 2)


def remote(src, dst, send_sem, recv_sem, device):
    return pltpu.make_async_remote_copy(
        src_ref=src, dst_ref=dst, send_sem=send_sem, recv_sem=recv_sem,
        device_id=device, device_id_type=MESH,
    )


def layer_norm(cells, gain, bias):
    mean = jnp.mean(cells, -1, keepdims=True)
    centred = cells - mean
    variance = jnp.mean(centred * centred, -1, keepdims=True)
    return centred * lax.rsqrt(variance + EPS) * gain + bias


def kernel(
    n_sp, cap,
    resid, queries, keys, values, docs, sinks, out_proj_hbm, gain1, bias1,
    route_ids, route_weights, gate_hbm, up_hbm, down_hbm, gain2, bias2,
    out,
    gate, up, down, out_proj, kk, vv, doc_own, doc_halo, attended,
    proj_part, proj_in, proj_left, proj_right, normed,
    wide, table, arrived, rows, hidden, part, sum_in, from_left, from_right,
    result, returned, acc,
    load_sems, halo_send, halo_recv, proj_send, proj_recv,
    chain, paired, cross, present, z_send, z_recv, ag_send, ag_recv, rs_send, rs_recv, back_send, back_recv,
):
    sp = lax.axis_index("sp")
    tp = lax.axis_index("tp")
    n_tp = 4
    nz = n_sp // 2
    z, core = sp // 2, sp % 2
    right, left = (tp + 1) % n_tp, (tp + n_tp - 1) % n_tp
    to_right, to_left = {"tp": right}, {"tp": left}
    last = n_sp - 1
    partner = sp + 1 - 2 * core
    across = sp - 1 + 2 * core
    has_across = (across >= 0) & (across <= last)
    seat = (z - 1 + nz) % nz
    is_late = seat >= nz - 2
    mate = {"sp": core + 2 * (nz - 1) - 2 * jnp.where(z == 0, 0, nz - 1)}
    tok_dev = queries.shape[0]
    tok_sub, width = resid.shape
    cut = width // LANES
    unit = cap * cut
    own_pad = kk.shape[0] - 2 * WINDOW
    spans = [(2 * first, 2 * (end - first)) for first, end in groups_of(nz)]

    def row_device(row):
        return {"sp": 2 * row + core}

    def seated(p, c):
        return 2 * ((p + 1) % nz) + c

    def region(g, part_of=None):
        start, slots = spans[g]
        if part_of is None:
            return pl.ds(start * unit, slots * unit)
        return pl.ds((start + part_of * (slots // 2)) * unit, slots // 2 * unit)


    loads = [
        pltpu.make_async_copy(out_proj_hbm, out_proj, load_sems.at[0]),
        pltpu.make_async_copy(gate_hbm.at[0], gate, load_sems.at[1]),
        pltpu.make_async_copy(up_hbm.at[0], up, load_sems.at[2]),
        pltpu.make_async_copy(down_hbm.at[0], down, load_sems.at[3]),
    ]

    barrier = pltpu.get_barrier_semaphore()

    def tell(sem, device):
        pl.semaphore_signal(sem, inc=1, device_id=device, device_id_type=MESH)

    tell(barrier, to_right)
    tell(barrier, to_left)
    @pl.when(core == 1)
    def _():
        tell(barrier, {"sp": partner})

    @pl.when(has_across)
    def _():
        tell(barrier, {"sp": across})

    @pl.when((seat > 0) & jnp.logical_not(is_late))
    def _():
        tell(barrier, row_device(z - 1))

    @pl.when(is_late)
    def _():
        tell(barrier, row_device(nz - 2))

    @pl.when(z == 0)
    def _():
        tell(barrier, mate)

    for load in loads:
        load.start()

    def doubled(cells):
        return jnp.transpose(jnp.concatenate([cells, cells], axis=0).astype(F32)).astype(BF16)

    kk[pl.ds(0, tok_dev), :] = doubled(keys[...])
    vv[pl.ds(0, tok_dev), :] = doubled(values[...])
    if own_pad > tok_dev:
        pad = jnp.zeros((own_pad - tok_dev, LANES), BF16)
        kk[pl.ds(tok_dev, own_pad - tok_dev), :] = pad
        vv[pl.ds(tok_dev, own_pad - tok_dev), :] = pad
    doc_own[...] = jnp.broadcast_to(docs[...], doc_own.shape)

    prev_slot, next_slot = pl.ds(own_pad, WINDOW), pl.ds(own_pad + WINDOW, WINDOW)

    def blank(slot, i):
        kk[slot, :] = jnp.zeros((WINDOW, LANES), BF16)
        vv[slot, :] = jnp.zeros((WINDOW, LANES), BF16)
        doc_halo[i] = jnp.zeros(doc_own.shape, jnp.int32)

    @pl.when(sp == 0)
    def _():
        blank(prev_slot, 0)

    @pl.when(sp == last)
    def _():
        blank(next_slot, 1)

    expected = 3 + jnp.where(core == 0, 1, 0) + jnp.where(has_across, 1, 0)
    pl.semaphore_wait(barrier, expected + jnp.where(seat == nz - 3, 1, 0) - jnp.where(z == 0, 1, 0))

    tail = pl.ds(tok_dev - WINDOW, WINDOW)
    head = pl.ds(0, WINDOW)
    to_next, to_prev = {"sp": (sp + 1) % n_sp}, {"sp": (sp + last) % n_sp}
    halos_up = [
        remote(src, dst, halo_send.at[i], halo_recv.at[i], to_next)
        for i, (src, dst) in enumerate([
            (doc_own, doc_halo.at[0]), (kk.at[tail], kk.at[prev_slot]), (vv.at[tail], vv.at[prev_slot]),
        ])
    ]
    halos_down = [
        remote(src, dst, halo_send.at[i], halo_recv.at[i], to_prev)
        for i, (src, dst) in enumerate([
            (doc_own, doc_halo.at[1]), (kk.at[head], kk.at[next_slot]), (vv.at[head], vv.at[next_slot]),
        ], 3)
    ]

    @pl.when(core == 0)
    def _():
        tell(paired, {"sp": partner})

    @pl.when(sp < last)
    def _():
        for copy in halos_up:
            copy.start()

    @pl.when(core == 1)
    def _():
        pl.semaphore_wait(paired, 1)

    @pl.when(sp > 0)
    def _():
        for copy in halos_down:
            copy.start()

    def tell_earlier(p, carry):
        for c in range(2):
            tell(present.at[sp], {"sp": seated(p, c)})
        return carry

    @pl.when(z > 0)
    def _():
        @pl.when(seat > 0)
        def _():
            pl.semaphore_wait(chain, 1)

        @pl.when(seat < nz - 3)
        def _():
            tell(chain, row_device(z + 1))

        @pl.when(seat == nz - 3)
        def _():
            tell(chain, row_device(nz - 1))
            tell(chain, row_device(0))

        @pl.when(z == nz - 1)
        def _():
            tell(cross, mate)

        lax.fori_loop(0, jnp.minimum(seat, nz - 2), tell_earlier, 0)

    ids = route_ids[...].astype(F32)
    sub_i = lax.broadcasted_iota(jnp.int32, (tok_sub, tok_sub), 0)
    lane_i = lax.broadcasted_iota(jnp.int32, (tok_sub, tok_sub), 1)

    def upright(row):
        return jnp.sum(jnp.where(sub_i == lane_i, row, 0.0), axis=1, keepdims=True)

    id_row = [ids[k : k + 1, :] for k in range(2)]
    id_col = [upright(row) for row in id_row]
    share = [upright(route_weights[k : k + 1, :]) for k in range(2)]
    slot_row, slot_col = [], []
    for k in range(2):
        row, col = cap * id_row[k], cap * id_col[k]
        for other in range(2):
            same_row = (id_col[other] == id_row[k]) & (sub_i < lane_i)
            row = row + jnp.sum(jnp.where(same_row, 1.0, 0.0), axis=0, keepdims=True)
            same_col = (id_col[k] == id_row[other]) & (lane_i < sub_i)
            col = col + jnp.sum(jnp.where(same_col, 1.0, 0.0), axis=1, keepdims=True)
        slot_row.append(row)
        slot_col.append(col)
    n_slots = n_sp * cap
    slot_sub = lax.broadcasted_iota(jnp.int32, (n_slots, tok_sub), 0).astype(F32)
    slot_lane = lax.broadcasted_iota(jnp.int32, (tok_sub, n_slots), 1).astype(F32)
    assign = jnp.where(
        (slot_sub == slot_row[0]) | (slot_sub == slot_row[1]), 1.0, 0.0
    ).astype(BF16)
    choose = [jnp.where(slot_lane == c, 1.0, 0.0).astype(BF16) for c in slot_col]

    reach = own_pad + 2 * WINDOW
    @pl.when(sp > 0)
    def _():
        for copy in halos_up:
            copy.wait_recv()

    @pl.when(sp < last)
    def _():
        for copy in halos_down:
            copy.wait_recv()

    doc_prev = doc_halo[0][0:1, :][:, tok_dev - WINDOW : tok_dev].astype(F32)
    doc_next = doc_halo[1][0:1, :][:, 0:WINDOW].astype(F32)
    doc_here = doc_own[0:1, :].astype(F32)
    if own_pad > tok_dev:
        doc_here = jnp.concatenate([doc_here, jnp.full((1, own_pad - tok_dev), -1.0, F32)], axis=1)
    doc_keys = jnp.concatenate([doc_here, doc_prev, doc_next], axis=1)
    q_sub = lax.broadcasted_iota(jnp.int32, (tok_dev, tok_dev), 0)
    q_lane = lax.broadcasted_iota(jnp.int32, (tok_dev, tok_dev), 1)
    doc_col = jnp.sum(
        jnp.where(q_sub == q_lane, doc_own[0:1, :].astype(F32), 0.0), axis=1, keepdims=True
    )
    lane = lax.broadcasted_iota(jnp.int32, (tok_dev, reach), 1)
    query = lax.broadcasted_iota(jnp.int32, (tok_dev, reach), 0)
    place = jnp.where(
        lane < own_pad, lane,
        jnp.where(lane < own_pad + WINDOW, lane - (own_pad + WINDOW), lane - (own_pad + WINDOW) + tok_dev),
    )
    at = place + sp * tok_dev
    allowed = (at >= 0) & (at < n_sp * tok_dev) & (jnp.abs(query - place) <= WINDOW)
    allowed = allowed & (doc_col == doc_keys)
    pair_lane = lax.broadcasted_iota(jnp.int32, (tok_dev, LANES), 1)
    for pair in range(queries.shape[1] // LANES):
        q_pair = queries[:, pair * LANES : (pair + 1) * LANES]
        outs = []
        for side in range(2):
            mine = (pair_lane < HEAD_DIM) if side == 0 else (pair_lane >= HEAD_DIM)
            q = jnp.where(mine, q_pair.astype(F32) * HEAD_DIM ** (-0.5), 0.0).astype(BF16)
            scores = lax.dot_general(
                q, kk[...], (((1,), (1,)), ((), ())), preferred_element_type=F32
            )
            scores = jnp.where(allowed, scores, MASKED)
            sink = sinks[2 * pair + side]
            top = jnp.maximum(jnp.max(scores, -1, keepdims=True), sink)
            raised = jnp.exp(scores - top)
            total = jnp.exp(sink - top) + jnp.sum(raised, -1, keepdims=True)
            weights = (raised * (1.0 / total)).astype(BF16)
            outs.append(jnp.dot(weights, vv[...], preferred_element_type=F32))
        attended[:, pair * LANES : (pair + 1) * LANES] = jnp.where(
            pair_lane < HEAD_DIM, outs[0], outs[1]
        ).astype(BF16)

    loads[0].wait()
    wide_half = width // 2
    opposite = (tp + 2) % n_tp

    def project(owner, j, h):
        block = attended[pl.ds(pl.multiple_of(owner * tok_sub, tok_sub), tok_sub), :]
        proj_part[j, h] = jnp.dot(
            block, out_proj[:, h * wide_half : (h + 1) * wide_half], preferred_element_type=F32
        ).astype(BF16)

    project(opposite, 3, 0)
    project(opposite, 3, 1)
    c_opp0 = remote(proj_part.at[3, 0], proj_in.at[0], proj_send.at[0], proj_recv.at[0], to_right)
    c_opp0.start()
    c_opp1 = remote(proj_part.at[3, 1], proj_in.at[1], proj_send.at[1], proj_recv.at[1], to_left)
    c_opp1.start()
    project(right, 2, 1)
    project(left, 1, 0)
    c_right1 = remote(proj_part.at[2, 1], proj_left.at[1], proj_send.at[2], proj_recv.at[2], to_right)
    c_right1.start()
    c_left0 = remote(proj_part.at[1, 0], proj_right.at[0], proj_send.at[3], proj_recv.at[3], to_left)
    c_left0.start()
    project(right, 2, 0)
    project(left, 1, 1)
    c_opp0.wait_recv()
    proj_part[2, 0] = (proj_part[2, 0].astype(F32) + proj_in[0].astype(F32)).astype(BF16)
    c_right0 = remote(proj_part.at[2, 0], proj_left.at[0], proj_send.at[4], proj_recv.at[4], to_right)
    c_right0.start()
    c_opp1.wait_recv()
    proj_part[1, 1] = (proj_part[1, 1].astype(F32) + proj_in[1].astype(F32)).astype(BF16)
    c_left1 = remote(proj_part.at[1, 1], proj_right.at[1], proj_send.at[5], proj_recv.at[5], to_left)
    c_left1.start()

    @pl.when(z == 0)
    def _():
        pl.semaphore_wait(chain, 1)
        pl.semaphore_wait(cross, 1)
        tell(cross, mate)
        lax.fori_loop(0, nz - 2, tell_earlier, 0)

    project(tp, 0, 0)
    project(tp, 0, 1)
    for copy in (c_right1, c_left0, c_right0, c_left1):
        copy.wait_recv()
    for h in range(2):
        cols = slice(h * wide_half, (h + 1) * wide_half)
        projected = (
            proj_part[0, h].astype(F32) + proj_left[h].astype(F32) + proj_right[h].astype(F32)
        ).astype(BF16)
        acc[:, cols] = ROOT2 * resid[:, cols].astype(F32) + projected.astype(F32)
    normed[...] = layer_norm(acc[...], gain1[...], bias1[...]).astype(BF16)

    for c in range(0, cut, 2):
        picked = jnp.dot(
            assign, normed[:, c * LANES : (c + 2) * LANES], preferred_element_type=F32
        )
        wide[pl.ds(c, n_slots, stride=cut), :] = picked[:, :LANES]
        wide[pl.ds(c + 1, n_slots, stride=cut), :] = picked[:, LANES:]
    for e in range(n_sp):
        table[e] = wide[pl.ds(e * unit, unit), :].astype(BF16)
    arrived[0, pl.ds(0, unit), :] = table[sp]

    def dispatch(g):
        def one(i, carry):
            o = jnp.where(i % 2 == 1, (i + 1) // 2, -(i // 2))
            zd = (z + o + nz) % nz
            place = pl.ds(pl.multiple_of((2 * i + core) * unit, unit), unit)
            for c in range(2):
                e = 2 * zd + c

                @pl.when(jnp.logical_not(is_late) & ((zd + nz - 1) % nz > seat))
                def _():
                    pl.semaphore_wait(present.at[e], 1)

                remote(
                    table.at[e], arrived.at[0, place], z_send.at[0], z_recv.at[g], {"sp": e}
                ).start()
            return carry

        start, slots = spans[g]
        lax.fori_loop(max(start // 2, 1), (start + slots) // 2, one, 0)

    @pl.when(z == nz - 1)
    def _():
        pl.semaphore_wait(cross, 1)

    remote(
        table.at[partner], arrived.at[0, pl.ds(unit, unit)], z_send.at[0], z_recv.at[0], {"sp": partner}
    ).start()
    dispatch(0)
    dispatch(1)

    ag_copies, rs_copies = [], []

    def ag(i, g, src, dst, device):
        copy = remote(src, dst, ag_send.at[i, g], ag_recv.at[i, g], device)
        ag_copies.append(copy)
        return copy

    def rs(i, g, src, dst, device):
        copy = remote(src, dst, rs_send.at[i, g], rs_recv.at[i, g], device)
        rs_copies.append(copy)
        return copy

    out_of = {}

    def step1(g):
        start, slots = spans[g]
        own = 1 if g == 0 else 0
        landed = arrived.at[0, pl.ds((start + own) * unit, (slots - own) * unit)]
        remote(landed, landed, z_send.at[0], z_recv.at[g], to_right).wait_recv()
        whole = region(g)
        a = ag(0, g, arrived.at[0, whole], arrived.at[1, whole], to_right)
        a.start()
        b = ag(1, g, arrived.at[0, whole], arrived.at[2, whole], to_left)
        b.start()
        out_of["one", g] = (a, b)

    def step2(g):
        a, b = out_of["one", g]
        first, second = region(g, 0), region(g, 1)
        a.wait_recv()
        c = ag(2, g, arrived.at[1, first], arrived.at[3, first], to_right)
        c.start()
        b.wait_recv()
        d = ag(3, g, arrived.at[2, second], arrived.at[3, second], to_left)
        d.start()
        out_of["two", g] = (c, d)

    def step3(g):
        first, second, whole = region(g, 0), region(g, 1), region(g)
        size = spans[g][1] * unit
        n_rows = n_tp * spans[g][1] * cap
        for copy in out_of["two", g]:
            copy.wait_recv()
        for j in range(n_tp):
            wide[pl.ds(j * size, size), :] = arrived[j, whole, :].astype(F32)
        for c in range(cut):
            rows[0:n_rows, c * LANES : (c + 1) * LANES] = wide[
                pl.ds(c, n_rows, stride=cut), :
            ].astype(BF16)
        if g == 0:
            loads[1].wait()
            loads[2].wait()
            loads[3].wait()
        step = min(256, hidden.shape[1])

        def act(n, carry):
            cols = pl.ds(pl.multiple_of(n * step, step), step)
            a = jnp.dot(rows[0:n_rows, :], gate[:, cols], preferred_element_type=F32)
            b = jnp.dot(rows[0:n_rows, :], up[:, cols], preferred_element_type=F32)
            hidden[0:n_rows, cols] = (a / (1.0 + jnp.exp(-a)) * b).astype(BF16)
            return carry

        lax.fori_loop(0, hidden.shape[1] // step, act, 0)
        for n in range(cut // 2):
            y = jnp.dot(
                hidden[0:n_rows, :], down[:, n * 256 : (n + 1) * 256], preferred_element_type=F32
            )
            wide[pl.ds(2 * n, n_rows, stride=cut), :] = y[:, :LANES]
            wide[pl.ds(2 * n + 1, n_rows, stride=cut), :] = y[:, LANES:]
        for j in (3, 1, 2, 0):
            part[j, whole, :] = wide[pl.ds(j * size, size), :].astype(BF16)
        a = rs(0, g, part.at[3, first], sum_in.at[first], to_right)
        b = rs(1, g, part.at[3, second], sum_in.at[second], to_left)
        c = rs(2, g, part.at[2, second], from_left.at[second], to_right)
        d = rs(3, g, part.at[1, first], from_right.at[first], to_left)
        for copy in (a, b, c, d):
            copy.start()
        out_of["three", g] = (a, b, c, d)

    def step4(g):
        a, b, c, d = out_of["three", g]
        first, second = region(g, 0), region(g, 1)
        a.wait_recv()
        part[2, first, :] = (part[2, first, :].astype(F32) + sum_in[first, :].astype(F32)).astype(BF16)
        e = rs(4, g, part.at[2, first], from_left.at[first], to_right)
        e.start()
        b.wait_recv()
        part[1, second, :] = (part[1, second, :].astype(F32) + sum_in[second, :].astype(F32)).astype(BF16)
        f = rs(5, g, part.at[1, second], from_right.at[second], to_left)
        f.start()
        out_of["four", g] = (c, d, e, f)

    def step5(g):
        whole = region(g)
        for copy in out_of["four", g]:
            copy.wait_recv()
        result[whole, :] = (
            part[0, whole, :].astype(F32) + from_left[whole, :].astype(F32) + from_right[whole, :].astype(F32)
        ).astype(BF16)
        start, slots = spans[g]
        for q in range(start, start + slots):
            src = pl.ds(q * unit, unit)
            if q == 0:
                returned[sp] = result[src, :]
            else:
                peer = partner if q == 1 else 2 * ((z - offset_of(q // 2) + nz) % nz) + q % 2
                remote(
                    result.at[src], returned.at[sp], back_send.at[0], back_recv.at[0], {"sp": peer}
                ).start()

    step1(0)
    dispatch(2)
    step2(0)
    step1(1)
    dispatch(3)
    step3(0)
    step2(1)
    step1(2)
    step4(0)
    step3(1)
    step2(2)
    step5(0)
    step4(1)
    step1(3)
    step3(2)
    step2(3)
    step5(1)
    step4(2)
    step3(3)
    step5(2)
    step4(3)
    step5(3)

    others = returned.at[pl.ds(0, last)]
    remote(others, others, back_send.at[0], back_recv.at[0], to_right).wait_recv()
    for e in range(n_sp):
        wide[pl.ds(e * unit, unit), :] = returned[e].astype(F32)
    for c in range(0, cut, 2):
        cols = slice(c * LANES, (c + 2) * LANES)
        cells = jnp.concatenate(
            [wide[pl.ds(c + i, n_slots, stride=cut), :].astype(BF16) for i in range(2)], axis=1
        )
        total = ROOT2 * normed[:, cols].astype(F32)
        moe = share[0] * jnp.dot(choose[0], cells, preferred_element_type=F32)
        moe = moe + share[1] * jnp.dot(choose[1], cells, preferred_element_type=F32)
        acc[:, cols] = total + moe
    out[...] = layer_norm(acc[...], gain2[...], bias2[...]).astype(BF16)

    @pl.when(sp < last)
    def _():
        for copy in halos_up:
            copy.wait_send()

    @pl.when(sp > 0)
    def _():
        for copy in halos_down:
            copy.wait_send()

    for copy in (c_opp0, c_opp1, c_right1, c_left0, c_right0, c_left1):
        copy.wait_send()
    for copy in ag_copies + rs_copies:
        copy.wait_send()
    remote(others, others, z_send.at[0], z_recv.at[0], to_right).wait_send()
    remote(others, others, back_send.at[0], back_recv.at[0], to_right).wait_send()


def per_device(
    resid, queries, keys, values, doc_ids, sink_logits, out_proj, norm1_gain, norm1_bias,
    route_ids, route_weights, expert_gate, expert_up, expert_down, norm2_gain, norm2_bias,
):
    n_sp = lax.axis_size("sp")
    tok_dev, att = queries.shape
    tok_sub, width = resid.shape
    ff = expert_gate.shape[2]
    cap = 2 * tok_sub // n_sp
    cut = width // LANES
    unit = cap * cut
    own_pad = -(-tok_dev // LANES) * LANES
    groups = len(groups_of(n_sp // 2))
    most = 2 * max(end - first for first, end in groups_of(n_sp // 2))
    n_rows = -(-4 * most * cap // 16) * 16
    vmem = pl.BlockSpec(memory_space=pltpu.VMEM)
    hbm = pl.BlockSpec(memory_space=pl.ANY)
    dma = pltpu.SemaphoreType.DMA
    scratch = [
        pltpu.VMEM((width, ff), BF16),
        pltpu.VMEM((width, ff), BF16),
        pltpu.VMEM((ff, width), BF16),
        pltpu.VMEM((att, width), BF16),
        pltpu.VMEM((own_pad + 2 * WINDOW, LANES), BF16),
        pltpu.VMEM((own_pad + 2 * WINDOW, LANES), BF16),
        pltpu.VMEM((8, tok_dev), jnp.int32),
        pltpu.VMEM((2, 8, tok_dev), jnp.int32),
        pltpu.VMEM((tok_dev, att), BF16),
        pltpu.VMEM((4, 2, tok_sub, width // 2), BF16),
        pltpu.VMEM((2, tok_sub, width // 2), BF16),
        pltpu.VMEM((2, tok_sub, width // 2), BF16),
        pltpu.VMEM((2, tok_sub, width // 2), BF16),
        pltpu.VMEM((tok_sub, width), BF16),
        pltpu.VMEM((max(n_sp, 4 * most) * unit, LANES), F32),
        pltpu.VMEM((n_sp, unit, LANES), BF16),
        pltpu.VMEM((4, n_sp * unit, LANES), BF16),
        pltpu.VMEM((n_rows, width), BF16),
        pltpu.VMEM((n_rows, ff), BF16),
        pltpu.VMEM((4, n_sp * unit, LANES), BF16),
        pltpu.VMEM((n_sp * unit, LANES), BF16),
        pltpu.VMEM((n_sp * unit, LANES), BF16),
        pltpu.VMEM((n_sp * unit, LANES), BF16),
        pltpu.VMEM((n_sp * unit, LANES), BF16),
        pltpu.VMEM((n_sp, unit, LANES), BF16),
        pltpu.VMEM((tok_sub, width), F32),
        dma((4,)), dma((6,)), dma((6,)), dma((6,)), dma((6,)),
        pltpu.SemaphoreType.REGULAR, pltpu.SemaphoreType.REGULAR,
        pltpu.SemaphoreType.REGULAR, pltpu.SemaphoreType.REGULAR((n_sp,)),
        dma((1,)), dma((groups,)), dma((4, groups)), dma((4, groups)),
        dma((6, groups)), dma((6, groups)), dma((1,)), dma((1,)),
    ]
    flops = 2 * tok_dev * att * width + 2 * 4 * tok_sub * 2 * width * ff * 3
    return pl.pallas_call(
        functools.partial(kernel, n_sp, cap),
        out_shape=jax.ShapeDtypeStruct((tok_sub, width), BF16),
        in_specs=[
            vmem, vmem, vmem, vmem, vmem, pl.BlockSpec(memory_space=pltpu.SMEM), hbm,
            vmem, vmem, vmem, vmem, hbm, hbm, hbm, vmem, vmem,
        ],
        out_specs=vmem,
        scratch_shapes=scratch,
        compiler_params=pltpu.CompilerParams(
            collective_id=0, has_side_effects=True, vmem_limit_bytes=56 * 1024 * 1024
        ),
        cost_estimate=pl.CostEstimate(flops=flops, bytes_accessed=12_000_000, transcendentals=0),
        name="layer",
    )(
        resid, queries, keys.T, values.T, doc_ids[None, :], sink_logits, out_proj,
        norm1_gain[None, :], norm1_bias[None, :], route_ids.T, route_weights.T,
        expert_gate, expert_up, expert_down, norm2_gain[None, :], norm2_bias[None, :],
    )


def solution(mesh):
    rows = ("grp", "sp", "tp")
    placed = (
        P(rows, None),
        P(("grp", "sp"), "tp"),
        P(("grp", "sp"), "tp"),
        P(("grp", "sp"), "tp"),
        P(("grp", "sp")),
        P("tp"),
        P("tp", None),
        P(),
        P(),
        P(rows, None),
        P(rows, None),
        P("sp", None, "tp"),
        P("sp", None, "tp"),
        P("sp", "tp", None),
        P(),
        P(),
    )
    return jax.shard_map(
        per_device, mesh=mesh, in_specs=placed, out_specs=P(rows, None), check_vma=False
    )
```

```python
import functools

import jax
import jax.numpy as jnp
from jax import lax
from jax.experimental import pallas as pl
from jax.experimental.pallas import tpu as pltpu
from jax.sharding import PartitionSpec as P

HEAD_DIM = 64
WINDOW = 128
LANES = 128
EPS = 1e-05
ROOT2 = 1.4142135623730951
MASKED = -1e30
MESH = pl.DeviceIdType.MESH
F32 = jnp.float32
BF16 = jnp.bfloat16


def groups_of(nz):
    base, extra = nz // 4, nz // 16
    edges = (0, base + extra, 2 * base + extra, 3 * base + extra, nz)
    return tuple(zip(edges[:-1], edges[1:]))


def offset_of(i):
    return (i + 1) // 2 if i % 2 else -(i // 2)


def remote(src, dst, send_sem, recv_sem, device):
    return pltpu.make_async_remote_copy(
        src_ref=src, dst_ref=dst, send_sem=send_sem, recv_sem=recv_sem,
        device_id=device, device_id_type=MESH,
    )


def layer_norm(cells, gain, bias):
    mean = jnp.mean(cells, -1, keepdims=True)
    centred = cells - mean
    variance = jnp.mean(centred * centred, -1, keepdims=True)
    return centred * lax.rsqrt(variance + EPS) * gain + bias


def kernel(
    n_sp, cap,
    resid, queries, keys, values, docs, sinks, out_proj_hbm, gain1, bias1,
    route_ids, route_weights, gate_hbm, up_hbm, down_hbm, gain2, bias2,
    out,
    gate, up, down, out_proj, kk, vv, doc_own, doc_halo, attended,
    proj_part, proj_in, proj_left, proj_right, normed,
    wide, table, arrived, rows, hidden, part, sum_in, from_left, from_right,
    result, returned, acc,
    load_sems, halo_send, halo_recv, proj_send, proj_recv,
    chain, paired, cross, present, z_send, z_recv, ag_send, ag_recv, rs_send, rs_recv, back_send, back_recv,
):
    sp = lax.axis_index("sp")
    tp = lax.axis_index("tp")
    n_tp = 4
    nz = n_sp // 2
    z, core = sp // 2, sp % 2
    right, left = (tp + 1) % n_tp, (tp + n_tp - 1) % n_tp
    to_right, to_left = {"tp": right}, {"tp": left}
    last = n_sp - 1
    partner = sp + 1 - 2 * core
    across = sp - 1 + 2 * core
    has_across = (across >= 0) & (across <= last)
    seat = (z - 1 + nz) % nz
    is_late = seat >= nz - 2
    mate = {"sp": core + 2 * (nz - 1) - 2 * jnp.where(z == 0, 0, nz - 1)}
    tok_dev = queries.shape[0]
    tok_sub, width = resid.shape
    cut = width // LANES
    unit = cap * cut
    own_pad = kk.shape[0] - 2 * WINDOW
    spans = [(2 * first, 2 * (end - first)) for first, end in groups_of(nz)]

    def row_device(row):
        return {"sp": 2 * row + core}

    def seated(p, c):
        return 2 * ((p + 1) % nz) + c

    def region(g, part_of=None):
        start, slots = spans[g]
        if part_of is None:
            return pl.ds(start * unit, slots * unit)
        return pl.ds((start + part_of * (slots // 2)) * unit, slots // 2 * unit)


    loads = [
        pltpu.make_async_copy(out_proj_hbm, out_proj, load_sems.at[0]),
        pltpu.make_async_copy(gate_hbm.at[0], gate, load_sems.at[1]),
        pltpu.make_async_copy(up_hbm.at[0], up, load_sems.at[2]),
        pltpu.make_async_copy(down_hbm.at[0], down, load_sems.at[3]),
    ]

    barrier = pltpu.get_barrier_semaphore()

    def tell(sem, device):
        pl.semaphore_signal(sem, inc=1, device_id=device, device_id_type=MESH)

    tell(barrier, to_right)
    tell(barrier, to_left)
    @pl.when(core == 1)
    def _():
        tell(barrier, {"sp": partner})

    @pl.when(has_across)
    def _():
        tell(barrier, {"sp": across})

    @pl.when((seat > 0) & jnp.logical_not(is_late))
    def _():
        tell(barrier, row_device(z - 1))

    @pl.when(is_late)
    def _():
        tell(barrier, row_device(nz - 2))

    @pl.when(z == 0)
    def _():
        tell(barrier, mate)

    for load in loads:
        load.start()

    def doubled(cells):
        return jnp.transpose(jnp.concatenate([cells, cells], axis=0).astype(F32)).astype(BF16)

    kk[pl.ds(0, tok_dev), :] = doubled(keys[...])
    vv[pl.ds(0, tok_dev), :] = doubled(values[...])
    if own_pad > tok_dev:
        pad = jnp.zeros((own_pad - tok_dev, LANES), BF16)
        kk[pl.ds(tok_dev, own_pad - tok_dev), :] = pad
        vv[pl.ds(tok_dev, own_pad - tok_dev), :] = pad
    doc_own[...] = jnp.broadcast_to(docs[...], doc_own.shape)

    prev_slot, next_slot = pl.ds(own_pad, WINDOW), pl.ds(own_pad + WINDOW, WINDOW)

    def blank(slot, i):
        kk[slot, :] = jnp.zeros((WINDOW, LANES), BF16)
        vv[slot, :] = jnp.zeros((WINDOW, LANES), BF16)
        doc_halo[i] = jnp.zeros(doc_own.shape, jnp.int32)

    @pl.when(sp == 0)
    def _():
        blank(prev_slot, 0)

    @pl.when(sp == last)
    def _():
        blank(next_slot, 1)

    expected = 3 + jnp.where(core == 0, 1, 0) + jnp.where(has_across, 1, 0)
    pl.semaphore_wait(barrier, expected + jnp.where(seat == nz - 3, 1, 0) - jnp.where(z == 0, 1, 0))

    tail = pl.ds(tok_dev - WINDOW, WINDOW)
    head = pl.ds(0, WINDOW)
    to_next, to_prev = {"sp": (sp + 1) % n_sp}, {"sp": (sp + last) % n_sp}
    halos_up = [
        remote(src, dst, halo_send.at[i], halo_recv.at[i], to_next)
        for i, (src, dst) in enumerate([
            (doc_own, doc_halo.at[0]), (kk.at[tail], kk.at[prev_slot]), (vv.at[tail], vv.at[prev_slot]),
        ])
    ]
    halos_down = [
        remote(src, dst, halo_send.at[i], halo_recv.at[i], to_prev)
        for i, (src, dst) in enumerate([
            (doc_own, doc_halo.at[1]), (kk.at[head], kk.at[next_slot]), (vv.at[head], vv.at[next_slot]),
        ], 3)
    ]

    @pl.when(core == 0)
    def _():
        tell(paired, {"sp": partner})

    @pl.when(sp < last)
    def _():
        for copy in halos_up:
            copy.start()

    @pl.when(core == 1)
    def _():
        pl.semaphore_wait(paired, 1)

    @pl.when(sp > 0)
    def _():
        for copy in halos_down:
            copy.start()

    def tell_earlier(p, carry):
        for c in range(2):
            tell(present.at[sp], {"sp": seated(p, c)})
        return carry

    @pl.when(z > 0)
    def _():
        @pl.when(seat > 0)
        def _():
            pl.semaphore_wait(chain, 1)

        @pl.when(seat < nz - 3)
        def _():
            tell(chain, row_device(z + 1))

        @pl.when(seat == nz - 3)
        def _():
            tell(chain, row_device(nz - 1))
            tell(chain, row_device(0))

        @pl.when(z == nz - 1)
        def _():
            tell(cross, mate)

        lax.fori_loop(0, jnp.minimum(seat, nz - 2), tell_earlier, 0)

    ids = route_ids[...].astype(F32)
    sub_i = lax.broadcasted_iota(jnp.int32, (tok_sub, tok_sub), 0)
    lane_i = lax.broadcasted_iota(jnp.int32, (tok_sub, tok_sub), 1)

    def upright(row):
        return jnp.sum(jnp.where(sub_i == lane_i, row, 0.0), axis=1, keepdims=True)

    id_row = [ids[k : k + 1, :] for k in range(2)]
    id_col = [upright(row) for row in id_row]
    share = [upright(route_weights[k : k + 1, :]) for k in range(2)]
    slot_row, slot_col = [], []
    for k in range(2):
        row, col = cap * id_row[k], cap * id_col[k]
        for other in range(2):
            same_row = (id_col[other] == id_row[k]) & (sub_i < lane_i)
            row = row + jnp.sum(jnp.where(same_row, 1.0, 0.0), axis=0, keepdims=True)
            same_col = (id_col[k] == id_row[other]) & (lane_i < sub_i)
            col = col + jnp.sum(jnp.where(same_col, 1.0, 0.0), axis=1, keepdims=True)
        slot_row.append(row)
        slot_col.append(col)
    n_slots = n_sp * cap
    slot_sub = lax.broadcasted_iota(jnp.int32, (n_slots, tok_sub), 0).astype(F32)
    slot_lane = lax.broadcasted_iota(jnp.int32, (tok_sub, n_slots), 1).astype(F32)
    assign = jnp.where(
        (slot_sub == slot_row[0]) | (slot_sub == slot_row[1]), 1.0, 0.0
    ).astype(BF16)
    choose = [jnp.where(slot_lane == c, 1.0, 0.0).astype(BF16) for c in slot_col]

    reach = own_pad + 2 * WINDOW
    @pl.when(sp > 0)
    def _():
        for copy in halos_up:
            copy.wait_recv()

    @pl.when(sp < last)
    def _():
        for copy in halos_down:
            copy.wait_recv()

    doc_prev = doc_halo[0][0:1, :][:, tok_dev - WINDOW : tok_dev].astype(F32)
    doc_next = doc_halo[1][0:1, :][:, 0:WINDOW].astype(F32)
    doc_here = doc_own[0:1, :].astype(F32)
    if own_pad > tok_dev:
        doc_here = jnp.concatenate([doc_here, jnp.full((1, own_pad - tok_dev), -1.0, F32)], axis=1)
    doc_keys = jnp.concatenate([doc_here, doc_prev, doc_next], axis=1)
    q_sub = lax.broadcasted_iota(jnp.int32, (tok_dev, tok_dev), 0)
    q_lane = lax.broadcasted_iota(jnp.int32, (tok_dev, tok_dev), 1)
    doc_col = jnp.sum(
        jnp.where(q_sub == q_lane, doc_own[0:1, :].astype(F32), 0.0), axis=1, keepdims=True
    )
    lane = lax.broadcasted_iota(jnp.int32, (tok_dev, reach), 1)
    query = lax.broadcasted_iota(jnp.int32, (tok_dev, reach), 0)
    place = jnp.where(
        lane < own_pad, lane,
        jnp.where(lane < own_pad + WINDOW, lane - (own_pad + WINDOW), lane - (own_pad + WINDOW) + tok_dev),
    )
    at = place + sp * tok_dev
    allowed = (at >= 0) & (at < n_sp * tok_dev) & (jnp.abs(query - place) <= WINDOW)
    allowed = allowed & (doc_col == doc_keys)
    pair_lane = lax.broadcasted_iota(jnp.int32, (tok_dev, LANES), 1)
    for pair in range(queries.shape[1] // LANES):
        q_pair = queries[:, pair * LANES : (pair + 1) * LANES]
        outs = []
        for side in range(2):
            mine = (pair_lane < HEAD_DIM) if side == 0 else (pair_lane >= HEAD_DIM)
            q = jnp.where(mine, q_pair.astype(F32) * HEAD_DIM ** (-0.5), 0.0).astype(BF16)
            scores = lax.dot_general(
                q, kk[...], (((1,), (1,)), ((), ())), preferred_element_type=F32
            )
            scores = jnp.where(allowed, scores, MASKED)
            sink = sinks[2 * pair + side]
            top = jnp.maximum(jnp.max(scores, -1, keepdims=True), sink)
            raised = jnp.exp(scores - top)
            total = jnp.exp(sink - top) + jnp.sum(raised, -1, keepdims=True)
            weights = (raised * (1.0 / total)).astype(BF16)
            outs.append(jnp.dot(weights, vv[...], preferred_element_type=F32))
        attended[:, pair * LANES : (pair + 1) * LANES] = jnp.where(
            pair_lane < HEAD_DIM, outs[0], outs[1]
        ).astype(BF16)

    loads[0].wait()
    wide_half = width // 2
    opposite = (tp + 2) % n_tp

    def project(owner, j, h):
        block = attended[pl.ds(pl.multiple_of(owner * tok_sub, tok_sub), tok_sub), :]
        proj_part[j, h] = jnp.dot(
            block, out_proj[:, h * wide_half : (h + 1) * wide_half], preferred_element_type=F32
        ).astype(BF16)

    project(opposite, 3, 0)
    project(opposite, 3, 1)
    c_opp0 = remote(proj_part.at[3, 0], proj_in.at[0], proj_send.at[0], proj_recv.at[0], to_right)
    c_opp0.start()
    c_opp1 = remote(proj_part.at[3, 1], proj_in.at[1], proj_send.at[1], proj_recv.at[1], to_left)
    c_opp1.start()
    project(right, 2, 1)
    project(left, 1, 0)
    c_right1 = remote(proj_part.at[2, 1], proj_left.at[1], proj_send.at[2], proj_recv.at[2], to_right)
    c_right1.start()
    c_left0 = remote(proj_part.at[1, 0], proj_right.at[0], proj_send.at[3], proj_recv.at[3], to_left)
    c_left0.start()
    project(right, 2, 0)
    project(left, 1, 1)
    c_opp0.wait_recv()
    proj_part[2, 0] = (proj_part[2, 0].astype(F32) + proj_in[0].astype(F32)).astype(BF16)
    c_right0 = remote(proj_part.at[2, 0], proj_left.at[0], proj_send.at[4], proj_recv.at[4], to_right)
    c_right0.start()
    c_opp1.wait_recv()
    proj_part[1, 1] = (proj_part[1, 1].astype(F32) + proj_in[1].astype(F32)).astype(BF16)
    c_left1 = remote(proj_part.at[1, 1], proj_right.at[1], proj_send.at[5], proj_recv.at[5], to_left)
    c_left1.start()

    @pl.when(z == 0)
    def _():
        pl.semaphore_wait(chain, 1)
        pl.semaphore_wait(cross, 1)
        tell(cross, mate)
        lax.fori_loop(0, nz - 2, tell_earlier, 0)

    project(tp, 0, 0)
    project(tp, 0, 1)
    for copy in (c_right1, c_left0, c_right0, c_left1):
        copy.wait_recv()
    for h in range(2):
        cols = slice(h * wide_half, (h + 1) * wide_half)
        projected = (
            proj_part[0, h].astype(F32) + proj_left[h].astype(F32) + proj_right[h].astype(F32)
        ).astype(BF16)
        acc[:, cols] = ROOT2 * resid[:, cols].astype(F32) + projected.astype(F32)
    normed[...] = layer_norm(acc[...], gain1[...], bias1[...]).astype(BF16)

    for c in range(0, cut, 2):
        picked = jnp.dot(
            assign, normed[:, c * LANES : (c + 2) * LANES], preferred_element_type=F32
        )
        wide[pl.ds(c, n_slots, stride=cut), :] = picked[:, :LANES]
        wide[pl.ds(c + 1, n_slots, stride=cut), :] = picked[:, LANES:]
    for e in range(n_sp):
        table[e] = wide[pl.ds(e * unit, unit), :].astype(BF16)
    arrived[0, pl.ds(0, unit), :] = table[sp]

    def dispatch(g):
        def one(i, carry):
            o = jnp.where(i % 2 == 1, (i + 1) // 2, -(i // 2))
            zd = (z + o + nz) % nz
            place = pl.ds(pl.multiple_of((2 * i + core) * unit, unit), unit)
            for c in range(2):
                e = 2 * zd + c

                @pl.when(jnp.logical_not(is_late) & ((zd + nz - 1) % nz > seat))
                def _():
                    pl.semaphore_wait(present.at[e], 1)

                remote(
                    table.at[e], arrived.at[0, place], z_send.at[g], z_recv.at[g], {"sp": e}
                ).start()
            return carry

        start, slots = spans[g]
        lax.fori_loop(max(start // 2, 1), (start + slots) // 2, one, 0)

    @pl.when(z == nz - 1)
    def _():
        pl.semaphore_wait(cross, 1)

    remote(
        table.at[partner], arrived.at[0, pl.ds(unit, unit)], z_send.at[0], z_recv.at[0], {"sp": partner}
    ).start()
    def sent(g):
        count = spans[g][1] - (1 if g == 0 else 0)
        cells = table.at[pl.ds(0, count)]
        remote(cells, cells, z_send.at[g], z_recv.at[g], to_right).wait_send()

    dispatch(0)
    sent(0)
    dispatch(1)

    ag_copies, rs_copies = [], []

    def ag(i, g, src, dst, device):
        copy = remote(src, dst, ag_send.at[i, g], ag_recv.at[i, g], device)
        ag_copies.append(copy)
        return copy

    def rs(i, g, src, dst, device):
        copy = remote(src, dst, rs_send.at[i, g], rs_recv.at[i, g], device)
        rs_copies.append(copy)
        return copy

    out_of = {}

    def step1(g):
        start, slots = spans[g]
        own = 1 if g == 0 else 0
        landed = arrived.at[0, pl.ds((start + own) * unit, (slots - own) * unit)]
        remote(landed, landed, z_send.at[0], z_recv.at[g], to_right).wait_recv()
        whole = region(g)
        a = ag(0, g, arrived.at[0, whole], arrived.at[1, whole], to_right)
        a.start()
        b = ag(1, g, arrived.at[0, whole], arrived.at[2, whole], to_left)
        b.start()
        out_of["one", g] = (a, b)

    def step2(g):
        a, b = out_of["one", g]
        first, second = region(g, 0), region(g, 1)
        a.wait_recv()
        c = ag(2, g, arrived.at[1, first], arrived.at[3, first], to_right)
        c.start()
        b.wait_recv()
        d = ag(3, g, arrived.at[2, second], arrived.at[3, second], to_left)
        d.start()
        out_of["two", g] = (c, d)

    def step3(g):
        first, second, whole = region(g, 0), region(g, 1), region(g)
        size = spans[g][1] * unit
        n_rows = n_tp * spans[g][1] * cap
        for copy in out_of["two", g]:
            copy.wait_recv()
        for j in range(n_tp):
            wide[pl.ds(j * size, size), :] = arrived[j, whole, :].astype(F32)
        for c in range(cut):
            rows[0:n_rows, c * LANES : (c + 1) * LANES] = wide[
                pl.ds(c, n_rows, stride=cut), :
            ].astype(BF16)
        if g == 0:
            loads[1].wait()
            loads[2].wait()
            loads[3].wait()
        step = min(256, hidden.shape[1])

        def act(n, carry):
            cols = pl.ds(pl.multiple_of(n * step, step), step)
            a = jnp.dot(rows[0:n_rows, :], gate[:, cols], preferred_element_type=F32)
            b = jnp.dot(rows[0:n_rows, :], up[:, cols], preferred_element_type=F32)
            hidden[0:n_rows, cols] = (a / (1.0 + jnp.exp(-a)) * b).astype(BF16)
            return carry

        lax.fori_loop(0, hidden.shape[1] // step, act, 0)
        for n in range(cut // 2):
            y = jnp.dot(
                hidden[0:n_rows, :], down[:, n * 256 : (n + 1) * 256], preferred_element_type=F32
            )
            wide[pl.ds(2 * n, n_rows, stride=cut), :] = y[:, :LANES]
            wide[pl.ds(2 * n + 1, n_rows, stride=cut), :] = y[:, LANES:]
        for j in (3, 1, 2, 0):
            part[j, whole, :] = wide[pl.ds(j * size, size), :].astype(BF16)
        a = rs(0, g, part.at[3, first], sum_in.at[first], to_right)
        b = rs(1, g, part.at[3, second], sum_in.at[second], to_left)
        c = rs(2, g, part.at[2, second], from_left.at[second], to_right)
        d = rs(3, g, part.at[1, first], from_right.at[first], to_left)
        for copy in (a, b, c, d):
            copy.start()
        out_of["three", g] = (a, b, c, d)

    def step4(g):
        a, b, c, d = out_of["three", g]
        first, second = region(g, 0), region(g, 1)
        a.wait_recv()
        part[2, first, :] = (part[2, first, :].astype(F32) + sum_in[first, :].astype(F32)).astype(BF16)
        e = rs(4, g, part.at[2, first], from_left.at[first], to_right)
        e.start()
        b.wait_recv()
        part[1, second, :] = (part[1, second, :].astype(F32) + sum_in[second, :].astype(F32)).astype(BF16)
        f = rs(5, g, part.at[1, second], from_right.at[second], to_left)
        f.start()
        out_of["four", g] = (c, d, e, f)

    def step5(g):
        whole = region(g)
        for copy in out_of["four", g]:
            copy.wait_recv()
        result[whole, :] = (
            part[0, whole, :].astype(F32) + from_left[whole, :].astype(F32) + from_right[whole, :].astype(F32)
        ).astype(BF16)
        start, slots = spans[g]
        for q in range(start, start + slots):
            src = pl.ds(q * unit, unit)
            if q == 0:
                returned[sp] = result[src, :]
            else:
                peer = partner if q == 1 else 2 * ((z - offset_of(q // 2) + nz) % nz) + q % 2
                remote(
                    result.at[src], returned.at[sp], back_send.at[0], back_recv.at[0], {"sp": peer}
                ).start()

    step1(0)
    dispatch(2)
    step2(0)
    step1(1)
    dispatch(3)
    step3(0)
    step2(1)
    step1(2)
    step4(0)
    step3(1)
    step2(2)
    step5(0)
    step4(1)
    step1(3)
    step3(2)
    step2(3)
    step5(1)
    step4(2)
    step3(3)
    step5(2)
    step4(3)
    step5(3)

    others = returned.at[pl.ds(0, last)]
    remote(others, others, back_send.at[0], back_recv.at[0], to_right).wait_recv()
    for e in range(n_sp):
        wide[pl.ds(e * unit, unit), :] = returned[e].astype(F32)
    for c in range(0, cut, 2):
        cols = slice(c * LANES, (c + 2) * LANES)
        cells = jnp.concatenate(
            [wide[pl.ds(c + i, n_slots, stride=cut), :].astype(BF16) for i in range(2)], axis=1
        )
        total = ROOT2 * normed[:, cols].astype(F32)
        moe = share[0] * jnp.dot(choose[0], cells, preferred_element_type=F32)
        moe = moe + share[1] * jnp.dot(choose[1], cells, preferred_element_type=F32)
        acc[:, cols] = total + moe
    out[...] = layer_norm(acc[...], gain2[...], bias2[...]).astype(BF16)

    @pl.when(sp < last)
    def _():
        for copy in halos_up:
            copy.wait_send()

    @pl.when(sp > 0)
    def _():
        for copy in halos_down:
            copy.wait_send()

    for copy in (c_opp0, c_opp1, c_right1, c_left0, c_right0, c_left1):
        copy.wait_send()
    for copy in ag_copies + rs_copies:
        copy.wait_send()
    for g in range(1, len(spans)):
        sent(g)
    remote(others, others, back_send.at[0], back_recv.at[0], to_right).wait_send()


def per_device(
    resid, queries, keys, values, doc_ids, sink_logits, out_proj, norm1_gain, norm1_bias,
    route_ids, route_weights, expert_gate, expert_up, expert_down, norm2_gain, norm2_bias,
):
    n_sp = lax.axis_size("sp")
    tok_dev, att = queries.shape
    tok_sub, width = resid.shape
    ff = expert_gate.shape[2]
    cap = 2 * tok_sub // n_sp
    cut = width // LANES
    unit = cap * cut
    own_pad = -(-tok_dev // LANES) * LANES
    groups = len(groups_of(n_sp // 2))
    most = 2 * max(end - first for first, end in groups_of(n_sp // 2))
    n_rows = -(-4 * most * cap // 16) * 16
    vmem = pl.BlockSpec(memory_space=pltpu.VMEM)
    hbm = pl.BlockSpec(memory_space=pl.ANY)
    dma = pltpu.SemaphoreType.DMA
    scratch = [
        pltpu.VMEM((width, ff), BF16),
        pltpu.VMEM((width, ff), BF16),
        pltpu.VMEM((ff, width), BF16),
        pltpu.VMEM((att, width), BF16),
        pltpu.VMEM((own_pad + 2 * WINDOW, LANES), BF16),
        pltpu.VMEM((own_pad + 2 * WINDOW, LANES), BF16),
        pltpu.VMEM((8, tok_dev), jnp.int32),
        pltpu.VMEM((2, 8, tok_dev), jnp.int32),
        pltpu.VMEM((tok_dev, att), BF16),
        pltpu.VMEM((4, 2, tok_sub, width // 2), BF16),
        pltpu.VMEM((2, tok_sub, width // 2), BF16),
        pltpu.VMEM((2, tok_sub, width // 2), BF16),
        pltpu.VMEM((2, tok_sub, width // 2), BF16),
        pltpu.VMEM((tok_sub, width), BF16),
        pltpu.VMEM((max(n_sp, 4 * most) * unit, LANES), F32),
        pltpu.VMEM((n_sp, unit, LANES), BF16),
        pltpu.VMEM((4, n_sp * unit, LANES), BF16),
        pltpu.VMEM((n_rows, width), BF16),
        pltpu.VMEM((n_rows, ff), BF16),
        pltpu.VMEM((4, n_sp * unit, LANES), BF16),
        pltpu.VMEM((n_sp * unit, LANES), BF16),
        pltpu.VMEM((n_sp * unit, LANES), BF16),
        pltpu.VMEM((n_sp * unit, LANES), BF16),
        pltpu.VMEM((n_sp * unit, LANES), BF16),
        pltpu.VMEM((n_sp, unit, LANES), BF16),
        pltpu.VMEM((tok_sub, width), F32),
        dma((4,)), dma((6,)), dma((6,)), dma((6,)), dma((6,)),
        pltpu.SemaphoreType.REGULAR, pltpu.SemaphoreType.REGULAR,
        pltpu.SemaphoreType.REGULAR, pltpu.SemaphoreType.REGULAR((n_sp,)),
        dma((groups,)), dma((groups,)), dma((4, groups)), dma((4, groups)),
        dma((6, groups)), dma((6, groups)), dma((1,)), dma((1,)),
    ]
    flops = 2 * tok_dev * att * width + 2 * 4 * tok_sub * 2 * width * ff * 3
    return pl.pallas_call(
        functools.partial(kernel, n_sp, cap),
        out_shape=jax.ShapeDtypeStruct((tok_sub, width), BF16),
        in_specs=[
            vmem, vmem, vmem, vmem, vmem, pl.BlockSpec(memory_space=pltpu.SMEM), hbm,
            vmem, vmem, vmem, vmem, hbm, hbm, hbm, vmem, vmem,
        ],
        out_specs=vmem,
        scratch_shapes=scratch,
        compiler_params=pltpu.CompilerParams(
            collective_id=0, has_side_effects=True, vmem_limit_bytes=56 * 1024 * 1024
        ),
        cost_estimate=pl.CostEstimate(flops=flops, bytes_accessed=12_000_000, transcendentals=0),
        name="layer",
    )(
        resid, queries, keys.T, values.T, doc_ids[None, :], sink_logits, out_proj,
        norm1_gain[None, :], norm1_bias[None, :], route_ids.T, route_weights.T,
        expert_gate, expert_up, expert_down, norm2_gain[None, :], norm2_bias[None, :],
    )


def solution(mesh):
    rows = ("grp", "sp", "tp")
    placed = (
        P(rows, None),
        P(("grp", "sp"), "tp"),
        P(("grp", "sp"), "tp"),
        P(("grp", "sp"), "tp"),
        P(("grp", "sp")),
        P("tp"),
        P("tp", None),
        P(),
        P(),
        P(rows, None),
        P(rows, None),
        P("sp", None, "tp"),
        P("sp", None, "tp"),
        P("sp", "tp", None),
        P(),
        P(),
    )
    return jax.shard_map(
        per_device, mesh=mesh, in_specs=placed, out_specs=P(rows, None), check_vma=False
    )
```

```python
import functools

import jax
import jax.numpy as jnp
from jax import lax
from jax.experimental import pallas as pl
from jax.experimental.pallas import tpu as pltpu
from jax.sharding import PartitionSpec as P

HEAD_DIM = 64
WINDOW = 128
LANES = 128
EPS = 1e-05
ROOT2 = 1.4142135623730951
MASKED = -1e30
MESH = pl.DeviceIdType.MESH
F32 = jnp.float32
BF16 = jnp.bfloat16


def groups_of(nz):
    base, extra = nz // 4, nz // 16
    one, two, three = base + extra, 2 * base + extra, 3 * base + extra
    return ((0, one), (one, two), (three, nz), (two, three))


def offset_of(i):
    return (i + 1) // 2 if i % 2 else -(i // 2)


def remote(src, dst, send_sem, recv_sem, device):
    return pltpu.make_async_remote_copy(
        src_ref=src, dst_ref=dst, send_sem=send_sem, recv_sem=recv_sem,
        device_id=device, device_id_type=MESH,
    )


def layer_norm(cells, gain, bias):
    mean = jnp.mean(cells, -1, keepdims=True)
    centred = cells - mean
    variance = jnp.mean(centred * centred, -1, keepdims=True)
    return centred * lax.rsqrt(variance + EPS) * gain + bias


def kernel(
    n_sp, cap,
    resid, queries, keys, values, docs, sinks, out_proj_hbm, gain1, bias1,
    route_ids, route_weights, gate_hbm, up_hbm, down_hbm, gain2, bias2,
    out,
    gate, up, down, out_proj, kk, vv, doc_own, doc_halo, attended,
    proj_part, proj_in, proj_left, proj_right, normed,
    wide, table, arrived, rows, hidden, part, sum_in, from_left, from_right,
    result, returned, acc,
    load_sems, halo_send, halo_recv, proj_send, proj_recv,
    chain, paired, cross, present, z_send, z_recv, ag_send, ag_recv, rs_send, rs_recv, back_send, back_recv,
):
    sp = lax.axis_index("sp")
    tp = lax.axis_index("tp")
    n_tp = 4
    nz = n_sp // 2
    z, core = sp // 2, sp % 2
    right, left = (tp + 1) % n_tp, (tp + n_tp - 1) % n_tp
    to_right, to_left = {"tp": right}, {"tp": left}
    last = n_sp - 1
    partner = sp + 1 - 2 * core
    across = sp - 1 + 2 * core
    has_across = (across >= 0) & (across <= last)
    seat = (z - 1 + nz) % nz
    is_late = seat >= nz - 2
    mate = {"sp": core + 2 * (nz - 1) - 2 * jnp.where(z == 0, 0, nz - 1)}
    tok_dev = queries.shape[0]
    tok_sub, width = resid.shape
    cut = width // LANES
    unit = cap * cut
    own_pad = kk.shape[0] - 2 * WINDOW
    spans = [(2 * first, 2 * (end - first)) for first, end in groups_of(nz)]

    def row_device(row):
        return {"sp": 2 * row + core}

    def seated(p, c):
        return 2 * ((p + 1) % nz) + c

    def region(g, part_of=None):
        start, slots = spans[g]
        if part_of is None:
            return pl.ds(start * unit, slots * unit)
        return pl.ds((start + part_of * (slots // 2)) * unit, slots // 2 * unit)


    loads = [
        pltpu.make_async_copy(out_proj_hbm, out_proj, load_sems.at[0]),
        pltpu.make_async_copy(gate_hbm.at[0], gate, load_sems.at[1]),
        pltpu.make_async_copy(up_hbm.at[0], up, load_sems.at[2]),
        pltpu.make_async_copy(down_hbm.at[0], down, load_sems.at[3]),
    ]

    barrier = pltpu.get_barrier_semaphore()

    def tell(sem, device):
        pl.semaphore_signal(sem, inc=1, device_id=device, device_id_type=MESH)

    tell(barrier, to_right)
    tell(barrier, to_left)
    @pl.when(core == 1)
    def _():
        tell(barrier, {"sp": partner})

    @pl.when(has_across)
    def _():
        tell(barrier, {"sp": across})

    @pl.when((seat > 0) & jnp.logical_not(is_late))
    def _():
        tell(barrier, row_device(z - 1))

    @pl.when(is_late)
    def _():
        tell(barrier, row_device(nz - 2))

    @pl.when(z == 0)
    def _():
        tell(barrier, mate)

    for load in loads:
        load.start()

    def doubled(cells):
        return jnp.transpose(jnp.concatenate([cells, cells], axis=0).astype(F32)).astype(BF16)

    kk[pl.ds(0, tok_dev), :] = doubled(keys[...])
    vv[pl.ds(0, tok_dev), :] = doubled(values[...])
    if own_pad > tok_dev:
        pad = jnp.zeros((own_pad - tok_dev, LANES), BF16)
        kk[pl.ds(tok_dev, own_pad - tok_dev), :] = pad
        vv[pl.ds(tok_dev, own_pad - tok_dev), :] = pad
    doc_own[...] = jnp.broadcast_to(docs[...], doc_own.shape)

    prev_slot, next_slot = pl.ds(own_pad, WINDOW), pl.ds(own_pad + WINDOW, WINDOW)

    def blank(slot, i):
        kk[slot, :] = jnp.zeros((WINDOW, LANES), BF16)
        vv[slot, :] = jnp.zeros((WINDOW, LANES), BF16)
        doc_halo[i] = jnp.zeros(doc_own.shape, jnp.int32)

    @pl.when(sp == 0)
    def _():
        blank(prev_slot, 0)

    @pl.when(sp == last)
    def _():
        blank(next_slot, 1)

    expected = 3 + jnp.where(core == 0, 1, 0) + jnp.where(has_across, 1, 0)
    pl.semaphore_wait(barrier, expected + jnp.where(seat == nz - 3, 1, 0) - jnp.where(z == 0, 1, 0))

    tail = pl.ds(tok_dev - WINDOW, WINDOW)
    head = pl.ds(0, WINDOW)
    to_next, to_prev = {"sp": (sp + 1) % n_sp}, {"sp": (sp + last) % n_sp}
    halos_up = [
        remote(src, dst, halo_send.at[i], halo_recv.at[i], to_next)
        for i, (src, dst) in enumerate([
            (doc_own, doc_halo.at[0]), (kk.at[tail], kk.at[prev_slot]), (vv.at[tail], vv.at[prev_slot]),
        ])
    ]
    halos_down = [
        remote(src, dst, halo_send.at[i], halo_recv.at[i], to_prev)
        for i, (src, dst) in enumerate([
            (doc_own, doc_halo.at[1]), (kk.at[head], kk.at[next_slot]), (vv.at[head], vv.at[next_slot]),
        ], 3)
    ]

    @pl.when(core == 0)
    def _():
        tell(paired, {"sp": partner})

    @pl.when(sp < last)
    def _():
        for copy in halos_up:
            copy.start()

    @pl.when(core == 1)
    def _():
        pl.semaphore_wait(paired, 1)

    @pl.when(sp > 0)
    def _():
        for copy in halos_down:
            copy.start()

    def tell_earlier(p, carry):
        for c in range(2):
            tell(present.at[sp], {"sp": seated(p, c)})
        return carry

    @pl.when(z > 0)
    def _():
        @pl.when(seat > 0)
        def _():
            pl.semaphore_wait(chain, 1)

        @pl.when(seat < nz - 3)
        def _():
            tell(chain, row_device(z + 1))

        @pl.when(seat == nz - 3)
        def _():
            tell(chain, row_device(nz - 1))
            tell(chain, row_device(0))

        @pl.when(z == nz - 1)
        def _():
            tell(cross, mate)

        lax.fori_loop(0, jnp.minimum(seat, nz - 2), tell_earlier, 0)

    ids = route_ids[...].astype(F32)
    sub_i = lax.broadcasted_iota(jnp.int32, (tok_sub, tok_sub), 0)
    lane_i = lax.broadcasted_iota(jnp.int32, (tok_sub, tok_sub), 1)

    def upright(row):
        return jnp.sum(jnp.where(sub_i == lane_i, row, 0.0), axis=1, keepdims=True)

    id_row = [ids[k : k + 1, :] for k in range(2)]
    id_col = [upright(row) for row in id_row]
    share = [upright(route_weights[k : k + 1, :]) for k in range(2)]
    slot_row, slot_col = [], []
    for k in range(2):
        row, col = cap * id_row[k], cap * id_col[k]
        for other in range(2):
            same_row = (id_col[other] == id_row[k]) & (sub_i < lane_i)
            row = row + jnp.sum(jnp.where(same_row, 1.0, 0.0), axis=0, keepdims=True)
            same_col = (id_col[k] == id_row[other]) & (lane_i < sub_i)
            col = col + jnp.sum(jnp.where(same_col, 1.0, 0.0), axis=1, keepdims=True)
        slot_row.append(row)
        slot_col.append(col)
    n_slots = n_sp * cap
    slot_sub = lax.broadcasted_iota(jnp.int32, (n_slots, tok_sub), 0).astype(F32)
    slot_lane = lax.broadcasted_iota(jnp.int32, (tok_sub, n_slots), 1).astype(F32)
    assign = jnp.where(
        (slot_sub == slot_row[0]) | (slot_sub == slot_row[1]), 1.0, 0.0
    ).astype(BF16)
    choose = [jnp.where(slot_lane == c, 1.0, 0.0).astype(BF16) for c in slot_col]

    reach = own_pad + 2 * WINDOW
    @pl.when(sp > 0)
    def _():
        for copy in halos_up:
            copy.wait_recv()

    @pl.when(sp < last)
    def _():
        for copy in halos_down:
            copy.wait_recv()

    doc_prev = doc_halo[0][0:1, :][:, tok_dev - WINDOW : tok_dev].astype(F32)
    doc_next = doc_halo[1][0:1, :][:, 0:WINDOW].astype(F32)
    doc_here = doc_own[0:1, :].astype(F32)
    if own_pad > tok_dev:
        doc_here = jnp.concatenate([doc_here, jnp.full((1, own_pad - tok_dev), -1.0, F32)], axis=1)
    doc_keys = jnp.concatenate([doc_here, doc_prev, doc_next], axis=1)
    q_sub = lax.broadcasted_iota(jnp.int32, (tok_dev, tok_dev), 0)
    q_lane = lax.broadcasted_iota(jnp.int32, (tok_dev, tok_dev), 1)
    doc_col = jnp.sum(
        jnp.where(q_sub == q_lane, doc_own[0:1, :].astype(F32), 0.0), axis=1, keepdims=True
    )
    lane = lax.broadcasted_iota(jnp.int32, (tok_dev, reach), 1)
    query = lax.broadcasted_iota(jnp.int32, (tok_dev, reach), 0)
    place = jnp.where(
        lane < own_pad, lane,
        jnp.where(lane < own_pad + WINDOW, lane - (own_pad + WINDOW), lane - (own_pad + WINDOW) + tok_dev),
    )
    at = place + sp * tok_dev
    allowed = (at >= 0) & (at < n_sp * tok_dev) & (jnp.abs(query - place) <= WINDOW)
    allowed = allowed & (doc_col == doc_keys)
    pair_lane = lax.broadcasted_iota(jnp.int32, (tok_dev, LANES), 1)
    for pair in range(queries.shape[1] // LANES):
        q_pair = queries[:, pair * LANES : (pair + 1) * LANES]
        outs = []
        for side in range(2):
            mine = (pair_lane < HEAD_DIM) if side == 0 else (pair_lane >= HEAD_DIM)
            q = jnp.where(mine, q_pair.astype(F32) * HEAD_DIM ** (-0.5), 0.0).astype(BF16)
            scores = lax.dot_general(
                q, kk[...], (((1,), (1,)), ((), ())), preferred_element_type=F32
            )
            scores = jnp.where(allowed, scores, MASKED)
            sink = sinks[2 * pair + side]
            top = jnp.maximum(jnp.max(scores, -1, keepdims=True), sink)
            raised = jnp.exp(scores - top)
            total = jnp.exp(sink - top) + jnp.sum(raised, -1, keepdims=True)
            weights = (raised * (1.0 / total)).astype(BF16)
            outs.append(jnp.dot(weights, vv[...], preferred_element_type=F32))
        attended[:, pair * LANES : (pair + 1) * LANES] = jnp.where(
            pair_lane < HEAD_DIM, outs[0], outs[1]
        ).astype(BF16)

    loads[0].wait()
    wide_half = width // 2
    opposite = (tp + 2) % n_tp

    def project(owner, j, h):
        block = attended[pl.ds(pl.multiple_of(owner * tok_sub, tok_sub), tok_sub), :]
        proj_part[j, h] = jnp.dot(
            block, out_proj[:, h * wide_half : (h + 1) * wide_half], preferred_element_type=F32
        ).astype(BF16)

    project(opposite, 3, 0)
    project(opposite, 3, 1)
    c_opp0 = remote(proj_part.at[3, 0], proj_in.at[0], proj_send.at[0], proj_recv.at[0], to_right)
    c_opp0.start()
    c_opp1 = remote(proj_part.at[3, 1], proj_in.at[1], proj_send.at[1], proj_recv.at[1], to_left)
    c_opp1.start()
    project(right, 2, 1)
    project(left, 1, 0)
    c_right1 = remote(proj_part.at[2, 1], proj_left.at[1], proj_send.at[2], proj_recv.at[2], to_right)
    c_right1.start()
    c_left0 = remote(proj_part.at[1, 0], proj_right.at[0], proj_send.at[3], proj_recv.at[3], to_left)
    c_left0.start()
    project(right, 2, 0)
    project(left, 1, 1)
    c_opp0.wait_recv()
    proj_part[2, 0] = (proj_part[2, 0].astype(F32) + proj_in[0].astype(F32)).astype(BF16)
    c_right0 = remote(proj_part.at[2, 0], proj_left.at[0], proj_send.at[4], proj_recv.at[4], to_right)
    c_right0.start()
    c_opp1.wait_recv()
    proj_part[1, 1] = (proj_part[1, 1].astype(F32) + proj_in[1].astype(F32)).astype(BF16)
    c_left1 = remote(proj_part.at[1, 1], proj_right.at[1], proj_send.at[5], proj_recv.at[5], to_left)
    c_left1.start()

    @pl.when(z == 0)
    def _():
        pl.semaphore_wait(chain, 1)
        pl.semaphore_wait(cross, 1)
        tell(cross, mate)
        lax.fori_loop(0, nz - 2, tell_earlier, 0)

    project(tp, 0, 0)
    project(tp, 0, 1)
    for copy in (c_right1, c_left0, c_right0, c_left1):
        copy.wait_recv()
    for h in range(2):
        cols = slice(h * wide_half, (h + 1) * wide_half)
        projected = (
            proj_part[0, h].astype(F32) + proj_left[h].astype(F32) + proj_right[h].astype(F32)
        ).astype(BF16)
        acc[:, cols] = ROOT2 * resid[:, cols].astype(F32) + projected.astype(F32)
    normed[...] = layer_norm(acc[...], gain1[...], bias1[...]).astype(BF16)

    for c in range(0, cut, 2):
        picked = jnp.dot(
            assign, normed[:, c * LANES : (c + 2) * LANES], preferred_element_type=F32
        )
        wide[pl.ds(c, n_slots, stride=cut), :] = picked[:, :LANES]
        wide[pl.ds(c + 1, n_slots, stride=cut), :] = picked[:, LANES:]
    for e in range(n_sp):
        table[e] = wide[pl.ds(e * unit, unit), :].astype(BF16)
    arrived[0, pl.ds(0, unit), :] = table[sp]

    def dispatch(g):
        def one(i, carry):
            o = jnp.where(i % 2 == 1, (i + 1) // 2, -(i // 2))
            zd = (z + o + nz) % nz
            place = pl.ds(pl.multiple_of((2 * i + core) * unit, unit), unit)
            for c in range(2):
                e = 2 * zd + c

                @pl.when(jnp.logical_not(is_late) & ((zd + nz - 1) % nz > seat))
                def _():
                    pl.semaphore_wait(present.at[e], 1)

                remote(
                    table.at[e], arrived.at[0, place], z_send.at[g], z_recv.at[g], {"sp": e}
                ).start()
            return carry

        start, slots = spans[g]
        lax.fori_loop(max(start // 2, 1), (start + slots) // 2, one, 0)

    @pl.when(z == nz - 1)
    def _():
        pl.semaphore_wait(cross, 1)

    remote(
        table.at[partner], arrived.at[0, pl.ds(unit, unit)], z_send.at[0], z_recv.at[0], {"sp": partner}
    ).start()
    def sent(g):
        count = spans[g][1] - (1 if g == 0 else 0)
        cells = table.at[pl.ds(0, count)]
        remote(cells, cells, z_send.at[g], z_recv.at[g], to_right).wait_send()

    dispatch(0)
    sent(0)
    dispatch(1)

    ag_copies, rs_copies = [], []

    def ag(i, g, src, dst, device):
        copy = remote(src, dst, ag_send.at[i, g], ag_recv.at[i, g], device)
        ag_copies.append(copy)
        return copy

    def rs(i, g, src, dst, device):
        copy = remote(src, dst, rs_send.at[i, g], rs_recv.at[i, g], device)
        rs_copies.append(copy)
        return copy

    out_of = {}

    def step1(g):
        start, slots = spans[g]
        own = 1 if g == 0 else 0
        landed = arrived.at[0, pl.ds((start + own) * unit, (slots - own) * unit)]
        remote(landed, landed, z_send.at[0], z_recv.at[g], to_right).wait_recv()
        whole = region(g)
        a = ag(0, g, arrived.at[0, whole], arrived.at[1, whole], to_right)
        a.start()
        b = ag(1, g, arrived.at[0, whole], arrived.at[2, whole], to_left)
        b.start()
        out_of["one", g] = (a, b)

    def step2(g):
        a, b = out_of["one", g]
        first, second = region(g, 0), region(g, 1)
        a.wait_recv()
        c = ag(2, g, arrived.at[1, first], arrived.at[3, first], to_right)
        c.start()
        b.wait_recv()
        d = ag(3, g, arrived.at[2, second], arrived.at[3, second], to_left)
        d.start()
        out_of["two", g] = (c, d)

    def step3(g):
        first, second, whole = region(g, 0), region(g, 1), region(g)
        size = spans[g][1] * unit
        n_rows = n_tp * spans[g][1] * cap
        for copy in out_of["two", g]:
            copy.wait_recv()
        for j in range(n_tp):
            wide[pl.ds(j * size, size), :] = arrived[j, whole, :].astype(F32)
        for c in range(cut):
            rows[0:n_rows, c * LANES : (c + 1) * LANES] = wide[
                pl.ds(c, n_rows, stride=cut), :
            ].astype(BF16)
        if g == 0:
            loads[1].wait()
            loads[2].wait()
            loads[3].wait()
        step = min(256, hidden.shape[1])

        def act(n, carry):
            cols = pl.ds(pl.multiple_of(n * step, step), step)
            a = jnp.dot(rows[0:n_rows, :], gate[:, cols], preferred_element_type=F32)
            b = jnp.dot(rows[0:n_rows, :], up[:, cols], preferred_element_type=F32)
            hidden[0:n_rows, cols] = (a / (1.0 + jnp.exp(-a)) * b).astype(BF16)
            return carry

        lax.fori_loop(0, hidden.shape[1] // step, act, 0)
        for n in range(cut // 2):
            y = jnp.dot(
                hidden[0:n_rows, :], down[:, n * 256 : (n + 1) * 256], preferred_element_type=F32
            )
            wide[pl.ds(2 * n, n_rows, stride=cut), :] = y[:, :LANES]
            wide[pl.ds(2 * n + 1, n_rows, stride=cut), :] = y[:, LANES:]
        for j in (3, 1, 2, 0):
            part[j, whole, :] = wide[pl.ds(j * size, size), :].astype(BF16)
        a = rs(0, g, part.at[3, first], sum_in.at[first], to_right)
        b = rs(1, g, part.at[3, second], sum_in.at[second], to_left)
        c = rs(2, g, part.at[2, second], from_left.at[second], to_right)
        d = rs(3, g, part.at[1, first], from_right.at[first], to_left)
        for copy in (a, b, c, d):
            copy.start()
        out_of["three", g] = (a, b, c, d)

    def step4(g):
        a, b, c, d = out_of["three", g]
        first, second = region(g, 0), region(g, 1)
        a.wait_recv()
        part[2, first, :] = (part[2, first, :].astype(F32) + sum_in[first, :].astype(F32)).astype(BF16)
        e = rs(4, g, part.at[2, first], from_left.at[first], to_right)
        e.start()
        b.wait_recv()
        part[1, second, :] = (part[1, second, :].astype(F32) + sum_in[second, :].astype(F32)).astype(BF16)
        f = rs(5, g, part.at[1, second], from_right.at[second], to_left)
        f.start()
        out_of["four", g] = (c, d, e, f)

    def step5(g):
        whole = region(g)
        for copy in out_of["four", g]:
            copy.wait_recv()
        result[whole, :] = (
            part[0, whole, :].astype(F32) + from_left[whole, :].astype(F32) + from_right[whole, :].astype(F32)
        ).astype(BF16)
        start, slots = spans[g]
        for q in range(start, start + slots):
            src = pl.ds(q * unit, unit)
            if q == 0:
                returned[sp] = result[src, :]
            else:
                peer = partner if q == 1 else 2 * ((z - offset_of(q // 2) + nz) % nz) + q % 2
                remote(
                    result.at[src], returned.at[sp], back_send.at[0], back_recv.at[0], {"sp": peer}
                ).start()

    step1(0)
    dispatch(2)
    step2(0)
    step1(1)
    dispatch(3)
    step3(0)
    step2(1)
    step1(2)
    step4(0)
    step3(1)
    step2(2)
    step5(0)
    step4(1)
    step1(3)
    step3(2)
    step2(3)
    step5(1)
    step4(2)
    step3(3)
    step5(2)
    step4(3)
    step5(3)

    others = returned.at[pl.ds(0, last)]
    remote(others, others, back_send.at[0], back_recv.at[0], to_right).wait_recv()
    for e in range(n_sp):
        wide[pl.ds(e * unit, unit), :] = returned[e].astype(F32)
    for c in range(0, cut, 2):
        cols = slice(c * LANES, (c + 2) * LANES)
        cells = jnp.concatenate(
            [wide[pl.ds(c + i, n_slots, stride=cut), :].astype(BF16) for i in range(2)], axis=1
        )
        total = ROOT2 * normed[:, cols].astype(F32)
        moe = share[0] * jnp.dot(choose[0], cells, preferred_element_type=F32)
        moe = moe + share[1] * jnp.dot(choose[1], cells, preferred_element_type=F32)
        acc[:, cols] = total + moe
    out[...] = layer_norm(acc[...], gain2[...], bias2[...]).astype(BF16)

    @pl.when(sp < last)
    def _():
        for copy in halos_up:
            copy.wait_send()

    @pl.when(sp > 0)
    def _():
        for copy in halos_down:
            copy.wait_send()

    for copy in (c_opp0, c_opp1, c_right1, c_left0, c_right0, c_left1):
        copy.wait_send()
    for copy in ag_copies + rs_copies:
        copy.wait_send()
    for g in range(1, len(spans)):
        sent(g)
    remote(others, others, back_send.at[0], back_recv.at[0], to_right).wait_send()


def per_device(
    resid, queries, keys, values, doc_ids, sink_logits, out_proj, norm1_gain, norm1_bias,
    route_ids, route_weights, expert_gate, expert_up, expert_down, norm2_gain, norm2_bias,
):
    n_sp = lax.axis_size("sp")
    tok_dev, att = queries.shape
    tok_sub, width = resid.shape
    ff = expert_gate.shape[2]
    cap = 2 * tok_sub // n_sp
    cut = width // LANES
    unit = cap * cut
    own_pad = -(-tok_dev // LANES) * LANES
    groups = len(groups_of(n_sp // 2))
    most = 2 * max(end - first for first, end in groups_of(n_sp // 2))
    n_rows = -(-4 * most * cap // 16) * 16
    vmem = pl.BlockSpec(memory_space=pltpu.VMEM)
    hbm = pl.BlockSpec(memory_space=pl.ANY)
    dma = pltpu.SemaphoreType.DMA
    scratch = [
        pltpu.VMEM((width, ff), BF16),
        pltpu.VMEM((width, ff), BF16),
        pltpu.VMEM((ff, width), BF16),
        pltpu.VMEM((att, width), BF16),
        pltpu.VMEM((own_pad + 2 * WINDOW, LANES), BF16),
        pltpu.VMEM((own_pad + 2 * WINDOW, LANES), BF16),
        pltpu.VMEM((8, tok_dev), jnp.int32),
        pltpu.VMEM((2, 8, tok_dev), jnp.int32),
        pltpu.VMEM((tok_dev, att), BF16),
        pltpu.VMEM((4, 2, tok_sub, width // 2), BF16),
        pltpu.VMEM((2, tok_sub, width // 2), BF16),
        pltpu.VMEM((2, tok_sub, width // 2), BF16),
        pltpu.VMEM((2, tok_sub, width // 2), BF16),
        pltpu.VMEM((tok_sub, width), BF16),
        pltpu.VMEM((max(n_sp, 4 * most) * unit, LANES), F32),
        pltpu.VMEM((n_sp, unit, LANES), BF16),
        pltpu.VMEM((4, n_sp * unit, LANES), BF16),
        pltpu.VMEM((n_rows, width), BF16),
        pltpu.VMEM((n_rows, ff), BF16),
        pltpu.VMEM((4, n_sp * unit, LANES), BF16),
        pltpu.VMEM((n_sp * unit, LANES), BF16),
        pltpu.VMEM((n_sp * unit, LANES), BF16),
        pltpu.VMEM((n_sp * unit, LANES), BF16),
        pltpu.VMEM((n_sp * unit, LANES), BF16),
        pltpu.VMEM((n_sp, unit, LANES), BF16),
        pltpu.VMEM((tok_sub, width), F32),
        dma((4,)), dma((6,)), dma((6,)), dma((6,)), dma((6,)),
        pltpu.SemaphoreType.REGULAR, pltpu.SemaphoreType.REGULAR,
        pltpu.SemaphoreType.REGULAR, pltpu.SemaphoreType.REGULAR((n_sp,)),
        dma((groups,)), dma((groups,)), dma((4, groups)), dma((4, groups)),
        dma((6, groups)), dma((6, groups)), dma((1,)), dma((1,)),
    ]
    flops = 2 * tok_dev * att * width + 2 * 4 * tok_sub * 2 * width * ff * 3
    return pl.pallas_call(
        functools.partial(kernel, n_sp, cap),
        out_shape=jax.ShapeDtypeStruct((tok_sub, width), BF16),
        in_specs=[
            vmem, vmem, vmem, vmem, vmem, pl.BlockSpec(memory_space=pltpu.SMEM), hbm,
            vmem, vmem, vmem, vmem, hbm, hbm, hbm, vmem, vmem,
        ],
        out_specs=vmem,
        scratch_shapes=scratch,
        compiler_params=pltpu.CompilerParams(
            collective_id=0, has_side_effects=True, vmem_limit_bytes=56 * 1024 * 1024
        ),
        cost_estimate=pl.CostEstimate(flops=flops, bytes_accessed=12_000_000, transcendentals=0),
        name="layer",
    )(
        resid, queries, keys.T, values.T, doc_ids[None, :], sink_logits, out_proj,
        norm1_gain[None, :], norm1_bias[None, :], route_ids.T, route_weights.T,
        expert_gate, expert_up, expert_down, norm2_gain[None, :], norm2_bias[None, :],
    )


def solution(mesh):
    rows = ("grp", "sp", "tp")
    placed = (
        P(rows, None),
        P(("grp", "sp"), "tp"),
        P(("grp", "sp"), "tp"),
        P(("grp", "sp"), "tp"),
        P(("grp", "sp")),
        P("tp"),
        P("tp", None),
        P(),
        P(),
        P(rows, None),
        P(rows, None),
        P("sp", None, "tp"),
        P("sp", None, "tp"),
        P("sp", "tp", None),
        P(),
        P(),
    )
    return jax.shard_map(
        per_device, mesh=mesh, in_specs=placed, out_specs=P(rows, None), check_vma=False
    )
```
